128 devices in a mesh: dp: 4 (over x), kv: 16 (over z, y), tp: 2 (over core).
Axes of the slice: x: 4, y: 4, z: 4, core: 2. Of those that a mesh axis runs over, the one named last changes fastest.
Arguments:
- tokens: bfloat16 [1024, 2048], P(('dp', 'kv', 'tp')), may hold values from -6 to 6
- norm_gain: float32 [2048], replicated, may hold values from 0.1 to 1.9
- gate_proj: bfloat16 [2048, 4096], P(None, ('kv', 'tp')), may hold values from -0.125 to 0.125
- inner_proj: bfloat16 [2048, 4096], P(None, ('kv', 'tp')), may hold values from -0.125 to 0.125
- write_proj: bfloat16 [2048, 1024], P(None, ('kv', 'tp')), may hold values from -0.125 to 0.125
- read_proj: bfloat16 [2048, 1024], P(None, ('kv', 'tp')), may hold values from -0.125 to 0.125
- step_proj: bfloat16 [2048, 64], replicated, may hold values from -0.125 to 0.125
- step_bias: float32 [64], replicated, may hold values from -3 to 0
- decay_log: float32 [64], replicated, may hold values from -5 to 0.7
- skip_gain: float32 [64], replicated, may hold values from 0.25 to 4
- conv_inner: bfloat16 [4, 4096], replicated, may hold values from -3 to 3
- conv_write: bfloat16 [4, 1024], replicated, may hold values from -3 to 3
- conv_read: bfloat16 [4, 1024], replicated, may hold values from -3 to 3
- out_gain: float32 [4096], replicated, may hold values from 0.1 to 1.9
- out_proj: bfloat16 [4096, 2048], P(('kv', 'tp')), may hold values from -0.09375 to 0.09375
- saved_state: float32 [256, 64, 64, 128], P('dp', ('kv', 'tp')), may hold values from -1.75 to 1.75
- inner_history: bfloat16 [256, 7, 4096], P('dp', None, ('kv', 'tp')), may hold values from -6 to 6
- write_history: bfloat16 [256, 7, 1024], P('dp', None, ('kv', 'tp')), may hold values from -6 to 6
- read_history: bfloat16 [256, 7, 1024], P('dp', None, ('kv', 'tp')), may hold values from -6 to 6
- last_steps: float32 [256, 4, 64], P('dp', None, ('kv', 'tp')), may hold values from 0.02 to 1
- accepted: int32 [256], P('dp'), may hold values from 0 to 4
Outputs:
- mixed: bfloat16 [1024, 2048], P(('dp', 'kv', 'tp'))
- base_state: float32 [256, 64, 64, 128], P('dp', ('kv', 'tp'))
The draws below stay inside these ranges and needn't reach their ends.
All inputs are finite; a program needn't handle non-finite values.
Results may differ from the reference program's by a relative error of at most 0.014.
Values may be sent and summed in bfloat16 or wider, within the bound.
No kernel may reach another device: no remote copies, remote signals or barrier semaphores. Data moves between devices by JAX's collectives and lax.ppermute only.
A program may use at most 64 MiB of HBM per device.

```python
import math
import jax
import jax.numpy as jnp
from jax import lax

D = 2048
HEADS = 64
HEAD_DIM = 64
STATE = 128
GROUPS = 8
WIDTH = 4
PROP = 4
INNER = 4096
SEQS = 256
TOKENS = 1024
HIST = 7


def draw_decay_log(key, part):
    spread_draw = jax.random.uniform(key, (HEADS,), jnp.float32)
    return -3.9 + 4.6 * spread_draw


def touch_ends(array, rng, least, largest):
    longest = array.shape.index(max(array.shape))
    spots = []
    for shift in (0, 1):
        where = [jax.random.randint(jax.random.fold_in(rng, axis), (), 0, length) for axis, length in enumerate(array.shape)]
        where[longest] = (where[longest] + shift) % array.shape[longest]
        spots.append(tuple(where))
    return array.at[spots[0]].set(least).at[spots[1]].set(largest)


def steps_of(rng, dims, pieces, low, high):
    factor_of = 1.0
    for axis_at, shards_of in pieces:
        draws = jax.random.uniform(jax.random.fold_in(jax.random.fold_in(rng, 6), axis_at), (shards_of,), jnp.float32, low / len(pieces), high / len(pieces))
        factor_of = factor_of * jnp.repeat(jnp.exp(draws), dims[axis_at] // shards_of).reshape((-1,) + (1,) * (len(dims) - 1 - axis_at))
    return factor_of


def normal_values(stream_key, extent, width, reach, shards=(), kind=jnp.bfloat16):
    factor_of = steps_of(stream_key, extent, shards, -0.22, 0.18) if shards else 1.0
    array = jax.random.normal(stream_key, extent, jnp.float32) * width * factor_of
    return jnp.minimum(jnp.maximum(array, -reach), reach).astype(kind)


def setup_inputs(seed: int = 0) -> dict:
    key_list = jax.random.split(jax.random.key(seed), 22)
    tokens = normal_values(key_list[0], (TOKENS, D), 1.0, 6.0, ((0, 128),))
    norm_gain = jnp.clip(1.0 + 0.18 * jax.random.normal(key_list[1], (D,), jnp.float32), 0.1, 1.9)
    gate_proj = normal_values(key_list[2], (D, INNER), D ** -0.5, 0.125, ((1, 32),))
    inner_proj = normal_values(key_list[3], (D, INNER), D ** -0.5, 0.125, ((1, 32),))
    write_proj = normal_values(key_list[4], (D, GROUPS * STATE), D ** -0.5, 0.125, ((1, 32),))
    read_proj = normal_values(key_list[5], (D, GROUPS * STATE), D ** -0.5, 0.125, ((1, 32),))
    step_proj = normal_values(key_list[6], (D, HEADS), D ** -0.5, 0.125)
    step_bias = jnp.clip(jax.random.uniform(key_list[7], (HEADS,), jnp.float32, -3.0, 0.0), -3.0, 0.0)
    decay_log = draw_decay_log(jax.random.fold_in(key_list[21], 71), 0)
    skip_gain = jnp.clip(jnp.exp(jax.random.uniform(key_list[9], (HEADS,), jnp.float32, math.log(0.25), math.log(4.0))), 0.25, 4.0)
    conv_inner = normal_values(key_list[10], (WIDTH, INNER), WIDTH ** -0.5, 3.0)
    conv_write = normal_values(key_list[11], (WIDTH, GROUPS * STATE), WIDTH ** -0.5, 3.0)
    conv_read = normal_values(key_list[12], (WIDTH, GROUPS * STATE), WIDTH ** -0.5, 3.0)
    out_gain = jnp.clip(1.0 + 0.18 * jax.random.normal(key_list[13], (INNER,), jnp.float32), 0.1, 1.9)
    out_proj = normal_values(key_list[14], (INNER, D), INNER ** -0.5, 0.09375, ((0, 32),))
    saved_state = normal_values(key_list[15], (SEQS, HEADS, HEAD_DIM, STATE), 0.3, 1.75, ((0, 4), (1, 32)), jnp.float32)
    inner_history = normal_values(key_list[16], (SEQS, HIST, INNER), 1.0, 6.0, ((0, 4), (2, 32)))
    write_history = normal_values(key_list[17], (SEQS, HIST, GROUPS * STATE), 1.0, 6.0, ((0, 4), (2, 32)))
    read_history = normal_values(key_list[18], (SEQS, HIST, GROUPS * STATE), 1.0, 6.0, ((0, 4), (2, 32)))
    last_steps = jnp.clip(jnp.exp(math.log(1.0) - 3.912023 * jax.random.uniform(key_list[19], (SEQS, PROP, HEADS), jnp.float32) ** steps_of(key_list[19], (SEQS, PROP, HEADS), ((0, 4), (2, 32)), -0.2, 0.2)), 0.02, 1.0)
    accepted = touch_ends(jax.random.randint(key_list[20], (SEQS,), 0, PROP + 1), jax.random.fold_in(key_list[20], 1), 0, PROP).astype(jnp.int32)
    return {"tokens": tokens, "norm_gain": norm_gain, "gate_proj": gate_proj, "inner_proj": inner_proj, "write_proj": write_proj, "read_proj": read_proj, "step_proj": step_proj, "step_bias": step_bias, "decay_log": decay_log, "skip_gain": skip_gain, "conv_inner": conv_inner, "conv_write": conv_write, "conv_read": conv_read, "out_gain": out_gain, "out_proj": out_proj, "saved_state": saved_state, "inner_history": inner_history, "write_history": write_history, "read_history": read_history, "last_steps": last_steps, "accepted": accepted}


EPSILON = 0.1
highest = lax.Precision.HIGHEST

def conv_rows(row_block, weight):
    out_len = row_block.shape[1] - weight.shape[0] + 1
    result = weight[0] * row_block[:, 0:out_len]
    for offset in range(1, weight.shape[0]):
        result = result + weight[offset] * row_block[:, offset:offset + out_len]
    return result

def rounded(values):
    return lax.optimization_barrier(values.astype(jnp.bfloat16)).astype(jnp.float32)

def reference(tokens, norm_gain, gate_proj, inner_proj, write_proj, read_proj, step_proj, step_bias, decay_log, skip_gain, conv_inner, conv_write, conv_read, out_gain, out_proj, saved_state, inner_history, write_history, read_history, last_steps, accepted):
    seq_count = saved_state.shape[0]
    own_rows = tokens.astype(jnp.float32)
    normed = (own_rows * lax.rsqrt(lax.optimization_barrier(jnp.mean(own_rows * own_rows, axis=-1, keepdims=True)) + EPSILON) * norm_gain).astype(jnp.bfloat16)
    gate_rows = jnp.dot(normed, gate_proj, preferred_element_type=jnp.float32).astype(jnp.bfloat16)
    inner_rows = jnp.dot(normed, inner_proj, preferred_element_type=jnp.float32).astype(jnp.bfloat16)
    write_rows = jnp.dot(normed, write_proj, preferred_element_type=jnp.float32).astype(jnp.bfloat16)
    read_rows = jnp.dot(normed, read_proj, preferred_element_type=jnp.float32).astype(jnp.bfloat16)
    step_rows = jnp.dot(normed, step_proj, preferred_element_type=jnp.float32)
    conv_width = conv_inner.shape[0]
    window_rows = (accepted[:, None] + jnp.arange(conv_width - 1, dtype=jnp.int32)[None, :]).astype(jnp.int32)

    def current(history, new_rows, weight):
        window = jnp.take_along_axis(history, window_rows[:, :, None], axis=1)
        joined = jnp.concatenate([window, new_rows.reshape(seq_count, PROP, -1)], axis=1)
        return jax.nn.silu(conv_rows(joined.astype(jnp.float32), weight.astype(jnp.float32)))
    inner_old = jax.nn.silu(conv_rows(inner_history.astype(jnp.float32), conv_inner.astype(jnp.float32)))
    write_old = rounded(jax.nn.silu(conv_rows(write_history.astype(jnp.float32), conv_write.astype(jnp.float32))))
    inner_new = current(inner_history, inner_rows, conv_inner)
    write_new = rounded(current(write_history, write_rows, conv_write))
    read_new = rounded(current(read_history, read_rows, conv_read))
    step_size = jax.nn.softplus(step_rows + step_bias[None, :]).reshape(seq_count, PROP, HEADS)
    decay_rate = -jnp.exp(decay_log)
    per_group = HEADS // GROUPS
    accepted_mask = (jnp.arange(PROP, dtype=jnp.int32)[None, :] < accepted[:, None]).astype(jnp.float32)
    step_logs = decay_rate[None, None, :] * last_steps * accepted_mask[:, :, None]
    total_log = lax.optimization_barrier(jnp.sum(step_logs, axis=1))
    tail_log = total_log[:, None, :] - jnp.cumsum(step_logs, axis=1)
    old_weights = accepted_mask[:, :, None] * jnp.exp(tail_log) * last_steps
    inner_old_heads = inner_old.reshape(seq_count, PROP, HEADS, HEAD_DIM)
    write_old_heads = jnp.repeat(write_old.reshape(seq_count, PROP, GROUPS, STATE), per_group, axis=2)
    base_state = jnp.exp(total_log)[:, :, None, None] * saved_state + jnp.einsum('sth,sthp,sthn->shpn', old_weights, inner_old_heads, write_old_heads, precision=highest)
    cumulative = jnp.cumsum(decay_rate[None, None, :] * step_size, axis=1)
    log_gap = cumulative[:, :, None, :] - cumulative[:, None, :, :]
    causal = (jnp.arange(PROP)[:, None] >= jnp.arange(PROP)[None, :])[None, :, :, None]
    kernel = jnp.where(causal, jnp.exp(jnp.where(causal, log_gap, 0.0)), 0.0)
    write_heads = jnp.repeat(write_new.reshape(seq_count, PROP, GROUPS, STATE), per_group, axis=2)
    read_heads = jnp.repeat(read_new.reshape(seq_count, PROP, GROUPS, STATE), per_group, axis=2)
    scores = jnp.einsum('sihn,sjhn->sijh', read_heads, write_heads, precision=highest)
    inner_heads = inner_new.reshape(seq_count, PROP, HEADS, HEAD_DIM)
    within = jnp.einsum('sijh,sjh,sjhp->sihp', kernel * scores, step_size, inner_heads, precision=highest)
    carried = jnp.exp(cumulative)[..., None] * jnp.einsum('sihn,shpn->sihp', read_heads, base_state, precision=highest)
    mixed_heads = within + carried + skip_gain[None, None, :, None] * inner_heads
    gated_rows = mixed_heads.reshape(seq_count * PROP, INNER) * jax.nn.silu(gate_rows.astype(jnp.float32))
    squares = lax.optimization_barrier(jnp.mean(gated_rows * gated_rows, axis=-1, keepdims=True))
    unscaled = (gated_rows * out_gain).astype(jnp.bfloat16)
    mixed = (jnp.dot(unscaled, out_proj, preferred_element_type=jnp.float32) * lax.rsqrt(squares + EPSILON)).astype(jnp.bfloat16)
    return (mixed, base_state)
```

```python
import jax
import jax.numpy as jnp
from jax import lax
from jax.experimental import pallas as pl
from jax.experimental.pallas import tpu as pltpu
from jax.sharding import PartitionSpec as P


EPSILON = 0.1
INNER = 4096
f32 = jnp.float32
bf16 = jnp.bfloat16
NT = (((1,), (1,)), ((), ()))
NN = (((1,), (0,)), ((), ()))


def dot(a, b, dims=NN):
    return lax.dot_general(a, b, dims, preferred_element_type=f32)


def silu(x):
    return x * (1.0 / (1.0 + jnp.exp(-x)))


def fetch(pairs, sems):
    copies = [pltpu.make_async_copy(src, dst, sems.at[k]) for k, (src, dst) in enumerate(pairs)]
    for copy in copies:
        copy.start()
    return copies


def device_rank():
    return lax.axis_index("kv") * 2 + lax.axis_index("tp")


def begin_kernel(
    tok_hbm, w_hbm, r_hbm, wh_hbm, rh_hbm, all_ref, out_ref, tok_s, wh_s, rh_s, sems
):
    copies = fetch(
        (
            (tok_hbm, tok_s),
            (wh_hbm, wh_s),
            (rh_hbm, rh_s),
            (w_hbm, out_ref.at[0:32]),
            (r_hbm, out_ref.at[32:64]),
        ),
        sems,
    )
    copies[0].wait()
    for k in range(16):
        all_ref[k] = tok_s[...]
    copies[1].wait()
    copies[2].wait()
    for t in range(7):
        both = jnp.concatenate([wh_s[t].astype(f32), rh_s[t].astype(f32)], axis=1).astype(bf16)
        out_ref[64:80, t * 128 : (t + 1) * 128] = both[0:16]
        out_ref[64:80, (7 + t) * 128 : (8 + t) * 128] = both[16:32]
    out_ref[64:80, 1792:2048] = jnp.zeros((16, 256), bf16)
    copies[3].wait()
    copies[4].wait()


def windows(rows, acc):
    out = []
    for j in range(3):
        w = rows[j]
        for a in range(1, 5):
            w = jnp.where(acc == a, rows[a + j], w)
        out.append(w)
    return out


def old_parts(taps, w):
    return (
        taps[0] * w[0] + taps[1] * w[1] + taps[2] * w[2],
        taps[0] * w[1] + taps[1] * w[2],
        taps[0] * w[2],
    )


def prep_kernel(
    saved_hbm,
    ihist_hbm,
    tin_hbm,
    tw_hbm,
    tr_hbm,
    gain_hbm,
    ls_hbm,
    acc_hbm,
    decay_hbm,
    skip_hbm,
    bias_hbm,
    step_hbm,
    low_hbm,
    hin_ref,
    a_ref,
    tot_ref,
    acc_ref,
    wide_hbm,
    vec_ref,
    low_s,
    wide_s,
    saved_s,
    ihist_s,
    tin_s,
    tw_s,
    tr_s,
    gain_s,
    ls_s,
    acc_s,
    heads_s,
    step_s,
    sems,
    sent,
):
    rank = device_rank()
    head = rank * 2
    col = pl.multiple_of(rank * 128, 128)
    group = pl.multiple_of((rank >> 2) * 128, 128)
    small = (
        (acc_hbm, acc_s),
        (ls_hbm, ls_s),
        (decay_hbm, heads_s.at[0:1]),
        (skip_hbm, heads_s.at[1:2]),
        (bias_hbm, heads_s.at[2:3]),
        (tin_hbm.at[:, pl.ds(col, 128)], tin_s),
        (tw_hbm.at[:, pl.ds(group, 128)], tw_s),
        (tr_hbm.at[:, pl.ds(group, 128)], tr_s),
        (gain_hbm.at[:, pl.ds(col, 128)], gain_s),
        (ihist_hbm, ihist_s),
        (step_hbm, step_s),
    )
    big = tuple(
        (saved_hbm.at[k * 8 : (k + 1) * 8], saved_s.at[k * 8 : (k + 1) * 8]) for k in range(8)
    )
    copies = fetch(small + big, sems)
    for copy in copies[: len(small)]:
        copy.wait()

    tin = tin_s[...].astype(f32)
    vec_ref[0:4, :] = tin
    vec_ref[4:8, :] = tw_s[...].astype(f32)
    vec_ref[8:12, :] = tr_s[...].astype(f32)
    place = lax.broadcasted_iota(jnp.int32, (1, 64), 1)
    first = lax.broadcasted_iota(jnp.int32, (1, 128), 1) < 64

    def of_head(k, h):
        return jnp.sum(jnp.where(place == head + h, heads_s[k : k + 1], 0.0), axis=-1, keepdims=True)

    def spread(k):
        return jnp.where(first, of_head(k, 0), of_head(k, 1))

    vec_ref[12:13, :] = -jnp.exp(spread(0))
    vec_ref[13:14, :] = spread(1)
    vec_ref[14:15, :] = spread(2)
    vec_ref[15:16, :] = gain_s[...]

    acc_row = acc_s[...]
    acc = jnp.broadcast_to(acc_row.astype(f32), (128, 64)).T
    acc_ref[...] = acc
    rows = [ihist_s[t].astype(f32) for t in range(7)]
    taps = [tin[k : k + 1] for k in range(4)]
    for i, part in enumerate(old_parts(taps, windows(rows, acc))):
        hin_ref[i] = part

    def wide(pair):
        return jnp.concatenate([jnp.broadcast_to(v, (64, 64)) for v in pair], axis=0).T

    weights = [[], [], [], []]
    totals = []
    for h in range(2):
        rate = -jnp.exp(of_head(0, h))
        steps = [ls_s[t, h : h + 1, :] for t in range(4)]
        keep = [(acc_row > t).astype(f32) for t in range(4)]
        logs = [rate * steps[t] * keep[t] for t in range(4)]
        tail = jnp.zeros((1, 64), f32)
        for t in (3, 2, 1, 0):
            weights[t].append(keep[t] * jnp.exp(tail) * steps[t])
            tail = tail + logs[t]
        totals.append(jnp.exp(tail))
    tot_ref[...] = wide(totals)
    for t in range(4):
        a_ref[t] = silu(sum(taps[k] * rows[t + k] for k in range(4))) * wide(weights[t])

    pick = lax.broadcasted_iota(jnp.int32, (128, 64), 1) == (
        head + (lax.broadcasted_iota(jnp.int32, (128, 64), 0) >> 6)
    )
    wide_s[...] = dot(pick.astype(f32).astype(bf16), step_s[...]).astype(bf16)
    out = [pltpu.make_async_copy(wide_s, wide_hbm, sent.at[8])]
    out[0].start()
    for k in range(8):
        block = slice(k * 8, (k + 1) * 8)
        copies[len(small) + k].wait()
        low_s[block] = saved_s[block].astype(bf16)
        out.append(pltpu.make_async_copy(low_s.at[block], low_hbm.at[block], sent.at[k]))
        out[-1].start()
    for copy in out:
        copy.wait()


def group_kernel(p0_ref, p1_ref, p2_ref, p3_ref, acc_ref, vec_ref, wall_hbm, hwr_ref, b_ref, wall_s, hist_s, sems):
    member = device_rank() & 3
    for x, p in enumerate((p0_ref, p1_ref, p2_ref, p3_ref)):
        at = pl.multiple_of((member ^ x) * 32, 32)
        wall_s[pl.ds(at, 32), :] = p[0:32, :]
        wall_s[pl.ds(128 + at, 32), :] = p[32:64, :]
        for t in range(7):
            hist_s[t, pl.ds(at, 16), :] = p[64:80, t * 128 : (t + 1) * 128].astype(f32)
            hist_s[t, pl.ds(at + 16, 16), :] = p[64:80, (7 + t) * 128 : (8 + t) * 128].astype(f32)
    copy = pltpu.make_async_copy(wall_s, wall_hbm, sems.at[0])
    copy.start()
    both = [hist_s[t].T for t in range(7)]
    acc = acc_ref[...]
    acc2 = jnp.concatenate([acc, acc], axis=0)
    taps = [
        jnp.concatenate(
            [
                jnp.broadcast_to(vec_ref[4 + k : 5 + k, :], (64, 128)),
                jnp.broadcast_to(vec_ref[8 + k : 9 + k, :], (64, 128)),
            ],
            axis=0,
        )
        for k in range(4)
    ]
    for i, part in enumerate(old_parts(taps, windows(both, acc2))):
        hwr_ref[i] = part
    for t in range(4):
        w_old = silu(sum(vec_ref[4 + k : 5 + k, :] * both[t + k][0:64] for k in range(4)))
        b_ref[t] = w_old.astype(bf16).astype(f32)
    copy.wait()


def state_kernel(saved_hbm, a_ref, b_ref, tot_ref, after_ref, base_hbm, saved_s, base_s, sems, sent):
    blocks = [slice(k * 8, (k + 1) * 8) for k in range(8)]
    copies = fetch([(saved_hbm.at[k], saved_s.at[k]) for k in blocks], sems)
    tot = tot_ref[...]
    tot = jnp.concatenate([tot, tot], axis=0).T
    at = jnp.concatenate(
        [jnp.concatenate([a_ref[2 * p], a_ref[2 * p + 1]], axis=0).T for p in range(2)], axis=1
    ).astype(bf16)
    b = b_ref[...].reshape(256, 128).astype(bf16)
    lane = lax.broadcasted_iota(jnp.int32, (1, 256), 1) & 63
    out = []
    for k in range(8):
        copies[k].wait()
        for s in range(k * 8, (k + 1) * 8):
            mask = (lane == s).astype(f32).astype(bf16)
            base_s[s] = saved_s[s] * tot[:, s : s + 1] + dot(at * mask, b)
        copy = pltpu.make_async_copy(base_s.at[blocks[k]], base_hbm.at[blocks[k]], sent.at[k])
        copy.start()
        out.append(copy)
    for copy in out:
        copy.wait()


def main_kernel(
    mine_ref,
    other_ref,
    norm_hbm,
    gate_hbm,
    inner_hbm,
    step_hbm,
    wall_hbm,
    low_hbm,
    own_hbm,
    hin_ref,
    hwr_ref,
    vec_ref,
    a_ref,
    b_ref,
    tot_ref,
    keep_ref,
    give_ref,
    own_ref,
    norm_ref,
    gate_ref,
    inner_ref,
    step_ref,
    wall_ref,
    low_ref,
    nrm_s,
    rows_s,
    read_s,
    car_s,
    sems,
):
    copies = fetch(
        (
            (norm_hbm, norm_ref),
            (step_hbm, step_ref),
            (wall_hbm, wall_ref),
            (inner_hbm, inner_ref),
            (gate_hbm, gate_ref),
            (low_hbm, low_ref),
            (own_hbm, own_ref),
        ),
        sems,
    )
    copies[0].wait()
    core = lax.axis_index("tp")
    even = core == 0
    gain = norm_ref[...]
    for kv in range(16):
        a = mine_ref[kv].astype(f32)
        b = other_ref[kv].astype(f32)
        x = jnp.concatenate([jnp.where(even, a, b), jnp.where(even, b, a)], axis=0)
        scale = lax.rsqrt(jnp.mean(x * x, axis=-1, keepdims=True) + EPSILON)
        nrm_s[kv * 16 : (kv + 1) * 16, :] = (x * scale * gain).astype(bf16)
    normed = nrm_s[...]

    def rounded(v):
        return v.astype(bf16).astype(f32)

    for copy in copies[1:5]:
        copy.wait()
    rows_s[0] = dot(normed, step_ref[...], NT)
    fixed = rounded(dot(normed, wall_ref[...], NT))
    rows_s[1] = fixed[:, 0:128]
    rows_s[2] = fixed[:, 128:256]
    rows_s[3] = rounded(dot(normed, inner_ref[...]))
    rows_s[4] = rounded(dot(normed, gate_ref[...]))

    def at_time(t, k):
        return rows_s[k, pl.ds(t, 64, stride=4), :]

    def conv_new(new, parts, taps):
        out = []
        for i in range(4):
            v = taps[3] * new[i]
            for d in range(1, i + 1):
                v = v + taps[3 - d] * new[i - d]
            out.append(silu(v if i == 3 else v + parts[i]))
        return out

    def taps_of(first):
        return [vec_ref[first + k : first + k + 1, :] for k in range(4)]

    write = [at_time(t, 1) for t in range(4)]
    read = [at_time(t, 2) for t in range(4)]
    write = [rounded(v) for v in conv_new(write, [hwr_ref[i, 0:64] for i in range(3)], taps_of(4))]
    read = [
        rounded(v) for v in conv_new(read, [hwr_ref[i, 64:128] for i in range(3)], taps_of(8))
    ]
    for t in range(4):
        read_s[pl.ds(t, 64, stride=4), :] = read[t]
    copies[5].wait()
    quarter = lax.broadcasted_iota(jnp.int32, (16, 128), 0) >> 2
    for g in range(16):
        r = read_s[g * 16 : (g + 1) * 16, :].astype(bf16)
        st = low_ref[g * 4 : (g + 1) * 4].reshape(512, 128)
        full = dot(r, st, NT)
        v = full[:, 0:128]
        for q in range(1, 4):
            v = jnp.where(quarter == q, full[:, q * 128 : (q + 1) * 128], v)
        car_s[g * 16 : (g + 1) * 16, :] = v

    inner = conv_new([at_time(t, 3) for t in range(4)], [hin_ref[i] for i in range(3)], taps_of(0))
    rate = vec_ref[12:13, :]
    skip = vec_ref[13:14, :]
    bias = vec_ref[14:15, :]
    out_gain = vec_ref[15:16, :]
    steps = []
    for t in range(4):
        z = at_time(t, 0) + bias
        steps.append(jnp.maximum(z, 0.0) + jnp.log1p(jnp.exp(-jnp.abs(z))))
    sums = [rate * steps[0]]
    for t in range(1, 4):
        sums.append(sums[-1] + rate * steps[t])
    tot = tot_ref[...]
    moved = [steps[t] * inner[t] for t in range(4)]
    for i in range(4):
        state = tot * car_s[pl.ds(i, 64, stride=4), :]
        for t in range(4):
            state = state + a_ref[t] * jnp.sum(read[i] * b_ref[t], axis=-1, keepdims=True)
        y = jnp.exp(sums[i]) * state + skip * inner[i]
        for j in range(i + 1):
            score = jnp.sum(read[i] * write[j], axis=-1, keepdims=True)
            weight = score * jnp.exp(sums[i] - sums[j]) if j < i else score
            y = y + weight * moved[j]
        read_s[pl.ds(i, 64, stride=4), :] = y * silu(at_time(i, 4))

    def piece(kv, c):
        at = pl.multiple_of(kv * 16 + c * 8, 8)
        return read_s[pl.ds(at, 8), :]

    lane = lax.broadcasted_iota(jnp.int32, (16, 128), 1)
    for c, ref in ((core, keep_ref), (1 - core, give_ref)):
        for k in range(8):
            g = jnp.concatenate([piece(2 * k, c), piece(2 * k + 1, c)], axis=0)
            sq = jnp.sum(g * g, axis=-1, keepdims=True)
            hi = rounded(sq)
            ref[k * 16 : (k + 1) * 16, 0:128] = (g * out_gain).astype(bf16)
            ref[k * 16 : (k + 1) * 16, 128:256] = jnp.where(
                lane == 0, hi, jnp.where(lane == 1, sq - hi, 0.0)
            ).astype(bf16)
    copies[6].wait()


def out_kernel(keep_ref, got_ref, own_ref, other_ref, out_ref):
    value = dot(keep_ref[:, 0:128], own_ref[...]) + dot(got_ref[:, 0:128], other_ref[...])
    out_ref[:, 0:2048] = value.astype(bf16)
    both = keep_ref[:, 128:256].astype(f32) + got_ref[:, 128:256].astype(f32)
    sq = jnp.sum(both, axis=-1, keepdims=True)
    hi = sq.astype(bf16).astype(f32)
    lane = lax.broadcasted_iota(jnp.int32, (128, 128), 1)
    out_ref[:, 2048:2176] = jnp.where(lane == 0, hi, jnp.where(lane == 1, sq - hi, 0.0)).astype(bf16)


def sum_kernel(in_ref, out_ref):
    total = in_ref[0].astype(f32)
    for k in range(1, 16):
        total = total + in_ref[k].astype(f32)
    squares = jnp.sum(total[:, 2048:2176], axis=-1, keepdims=True)
    out_ref[...] = (total[:, 0:2048] * lax.rsqrt(squares / INNER + EPSILON)).astype(bf16)


def whole(memory_space=pltpu.VMEM):
    return pl.BlockSpec(memory_space=memory_space)


def swapped(value, axis):
    return lax.ppermute(value, axis, [(k, k ^ 1) for k in range(lax.axis_size(axis))])


def params(mib, **kw):
    return pltpu.CompilerParams(vmem_limit_bytes=mib << 20, **kw)


def body(
    tokens,
    norm_gain,
    gate_proj,
    inner_proj,
    write_proj,
    read_proj,
    step_proj,
    step_bias,
    decay_log,
    skip_gain,
    conv_inner,
    conv_write,
    conv_read,
    out_gain,
    out_proj,
    saved_state,
    inner_history,
    write_history,
    read_history,
    last_steps,
    accepted,
):
    def hbm(value):
        return pltpu.with_memory_space_constraint(value, pltpu.HBM)

    anywhere = whole(pl.ANY)
    dma = pltpu.SemaphoreType.DMA

    def shape(*dims, kind=f32):
        return jax.ShapeDtypeStruct(dims, kind)

    saved = saved_state.reshape(64, 128, 128)
    sent, pack = pl.pallas_call(
        begin_kernel,
        out_shape=[shape(16, 8, 2048, kind=bf16), shape(80, 2048, kind=bf16)],
        in_specs=[anywhere] * 5,
        out_specs=[whole()] * 2,
        scratch_shapes=[
            pltpu.VMEM((8, 2048), bf16),
            pltpu.VMEM((7, 32, 64), bf16),
            pltpu.VMEM((7, 32, 64), bf16),
            dma((5,)),
        ],
        compiler_params=params(4),
        name="begin",
    )(
        hbm(tokens),
        hbm(write_proj.T),
        hbm(read_proj.T),
        hbm(write_history.transpose(1, 2, 0)),
        hbm(read_history.transpose(1, 2, 0)),
    )
    mine = lax.all_to_all(sent, "kv", 0, 0, tiled=True)
    pack_kv = swapped(pack, "kv")
    pack_tp = swapped(pack, "tp")
    pack_both = swapped(pack_kv, "tp")
    out_other = swapped(out_proj, "tp")

    low, hin, a, tot, acc, step, vec = pl.pallas_call(
        prep_kernel,
        in_specs=[anywhere] * 12,
        out_specs=[anywhere] + [whole()] * 4 + [anywhere, whole()],
        out_shape=[
            pltpu.HBM((64, 128, 128), bf16),
            shape(3, 64, 128),
            shape(4, 64, 128),
            shape(64, 128),
            shape(64, 128),
            pltpu.HBM((128, 2048), bf16),
            shape(16, 128),
        ],
        scratch_shapes=[
            pltpu.VMEM((64, 128, 128), bf16),
            pltpu.VMEM((128, 2048), bf16),
            pltpu.VMEM((64, 128, 128), f32),
            pltpu.VMEM((7, 64, 128), bf16),
            pltpu.VMEM((4, 128), bf16),
            pltpu.VMEM((4, 128), bf16),
            pltpu.VMEM((4, 128), bf16),
            pltpu.VMEM((1, 128), f32),
            pltpu.VMEM((4, 2, 64), f32),
            pltpu.VMEM((1, 64), jnp.int32),
            pltpu.VMEM((3, 64), f32),
            pltpu.VMEM((64, 2048), bf16),
            dma((19,)),
            dma((9,)),
        ],
        compiler_params=params(12),
        name="prep",
    )(
        *[
            hbm(v)
            for v in (
                saved,
                inner_history.transpose(1, 0, 2),
                conv_inner,
                conv_write,
                conv_read,
                out_gain[None, :],
                last_steps.transpose(1, 2, 0),
                accepted[None, :],
                decay_log[None, :],
                skip_gain[None, :],
                step_bias[None, :],
                step_proj.T,
            )
        ]
    )
    wall, hwr, b = pl.pallas_call(
        group_kernel,
        in_specs=[whole()] * 6,
        out_specs=[anywhere] + [whole()] * 2,
        out_shape=[pltpu.HBM((256, 2048), bf16), shape(3, 128, 128), shape(4, 64, 128)],
        scratch_shapes=[pltpu.VMEM((256, 2048), bf16), pltpu.VMEM((7, 128, 128), f32), dma((1,))],
        compiler_params=params(6),
        name="group",
    )(pack, pack_tp, pack_kv, pack_both, acc, vec)

    other = swapped(mine, "tp")
    keep, give, own_proj = pl.pallas_call(
        main_kernel,
        in_specs=[whole()] * 2 + [anywhere] * 7 + [whole()] * 6,
        out_specs=[whole()] * 3,
        out_shape=[shape(128, 256, kind=bf16)] * 2 + [shape(128, 2048, kind=bf16)],
        scratch_shapes=[
            pltpu.VMEM((1, 2048), f32),
            pltpu.VMEM((2048, 128), bf16),
            pltpu.VMEM((2048, 128), bf16),
            pltpu.VMEM((128, 2048), bf16),
            pltpu.VMEM((256, 2048), bf16),
            pltpu.VMEM((64, 128, 128), bf16),
            pltpu.VMEM((256, 2048), bf16),
            pltpu.VMEM((5, 256, 128), f32),
            pltpu.VMEM((256, 128), f32),
            pltpu.VMEM((256, 128), f32),
            dma((7,)),
        ],
        compiler_params=params(20),
        name="main",
    )(
        mine,
        other,
        *[
            hbm(v)
            for v in (
                norm_gain[None, :],
                gate_proj,
                inner_proj,
                step,
                wall,
                low,
                out_proj,
            )
        ],
        hin,
        hwr,
        vec,
        a,
        b,
        tot,
    )
    got = swapped(give, "tp")
    partial = pl.pallas_call(
        out_kernel,
        in_specs=[whole()] * 4,
        out_specs=whole(),
        out_shape=shape(128, 2176, kind=bf16),
        compiler_params=params(6),
        name="project",
    )(keep, got, own_proj, out_other)
    arrived = lax.all_to_all(partial.reshape(16, 8, 2176), "kv", 0, 0, tiled=True)
    base = pl.pallas_call(
        state_kernel,
        in_specs=[anywhere] + [whole()] * 3 + [anywhere],
        out_specs=anywhere,
        out_shape=shape(64, 128, 128),
        scratch_shapes=[
            pltpu.VMEM((64, 128, 128), f32),
            pltpu.VMEM((64, 128, 128), f32),
            dma((8,)),
            dma((8,)),
        ],
        compiler_params=params(12),
        name="state",
    )(hbm(saved), a, b, tot, partial)
    mixed = pl.pallas_call(
        sum_kernel,
        in_specs=[whole()],
        out_specs=whole(),
        out_shape=shape(8, 2048, kind=bf16),
        compiler_params=params(4),
        name="total",
    )(arrived)
    return mixed, base.reshape(64, 2, 64, 128)


def solution(mesh):
    both = ("kv", "tp")
    placed = (
        P(("dp", "kv", "tp"), None),
        P(),
        P(None, both),
        P(None, both),
        P(None, both),
        P(None, both),
        P(),
        P(),
        P(),
        P(),
        P(),
        P(),
        P(),
        P(),
        P(both, None),
        P("dp", both, None, None),
        P("dp", None, both),
        P("dp", None, both),
        P("dp", None, both),
        P("dp", None, both),
        P("dp"),
    )
    return jax.shard_map(
        body,
        mesh=mesh,
        in_specs=placed,
        out_specs=(P(("dp", "kv", "tp"), None), P("dp", both, None, None)),
        check_vma=False,
    )
```

```python
import jax
import jax.numpy as jnp
from jax import lax
from jax.experimental import pallas as pl
from jax.experimental.pallas import tpu as pltpu
from jax.sharding import PartitionSpec as P


EPSILON = 0.1
INNER = 4096
f32 = jnp.float32
bf16 = jnp.bfloat16
NT = (((1,), (1,)), ((), ()))
NN = (((1,), (0,)), ((), ()))


def dot(a, b, dims=NN):
    return lax.dot_general(a, b, dims, preferred_element_type=f32)


def silu(x):
    return x * (1.0 / (1.0 + jnp.exp(-x)))


def fetch(pairs, sems):
    copies = [pltpu.make_async_copy(src, dst, sems.at[k]) for k, (src, dst) in enumerate(pairs)]
    for copy in copies:
        copy.start()
    return copies


def device_rank():
    return lax.axis_index("kv") * 2 + lax.axis_index("tp")


def begin_kernel(
    tok_hbm, w_hbm, r_hbm, wh_hbm, rh_hbm, all_hbm, out_ref, tok_s, wh_s, rh_s, sems, sent
):
    copies = fetch(
        (
            (tok_hbm, tok_s),
            (wh_hbm, wh_s),
            (rh_hbm, rh_s),
            (w_hbm, out_ref.at[0:32]),
            (r_hbm, out_ref.at[32:64]),
        ),
        sems,
    )
    copies[0].wait()
    out = fetch([(tok_s, all_hbm.at[k]) for k in range(16)], sent)
    copies[1].wait()
    copies[2].wait()
    for t in range(7):
        both = jnp.concatenate([wh_s[t].astype(f32), rh_s[t].astype(f32)], axis=1).astype(bf16)
        out_ref[64:80, t * 128 : (t + 1) * 128] = both[0:16]
        out_ref[64:80, (7 + t) * 128 : (8 + t) * 128] = both[16:32]
    out_ref[64:80, 1792:2048] = jnp.zeros((16, 256), bf16)
    for copy in copies[3:] + out:
        copy.wait()


def windows(rows, acc):
    out = []
    for j in range(3):
        w = rows[j]
        for a in range(1, 5):
            w = jnp.where(acc == a, rows[a + j], w)
        out.append(w)
    return out


def old_parts(taps, w):
    return (
        taps[0] * w[0] + taps[1] * w[1] + taps[2] * w[2],
        taps[0] * w[1] + taps[1] * w[2],
        taps[0] * w[2],
    )


def prep_kernel(
    saved_hbm,
    ihist_hbm,
    tin_hbm,
    tw_hbm,
    tr_hbm,
    gain_hbm,
    ls_hbm,
    acc_hbm,
    decay_hbm,
    skip_hbm,
    bias_hbm,
    step_hbm,
    keep_hbm,
    give_hbm,
    held_hbm,
    wide_hbm,
    acc_ref,
    vec_ref,
    sent_ref,
    held_s,
    low_s,
    wide_s,
    saved_s,
    ihist_s,
    tin_s,
    twin_s,
    tw_s,
    tr_s,
    gain_s,
    twin_gain_s,
    ls_s,
    acc_s,
    heads_s,
    step_s,
    sems,
    sent,
):
    rank = device_rank()
    core = rank & 1
    head = rank * 2
    col = pl.multiple_of(rank * 128, 128)
    twin_col = pl.multiple_of((rank ^ 1) * 128, 128)
    group = pl.multiple_of((rank >> 2) * 128, 128)
    small = (
        (acc_hbm, acc_s),
        (ls_hbm, ls_s),
        (decay_hbm, heads_s.at[0:1]),
        (skip_hbm, heads_s.at[1:2]),
        (bias_hbm, heads_s.at[2:3]),
        (tin_hbm.at[:, pl.ds(col, 128)], tin_s),
        (tin_hbm.at[:, pl.ds(twin_col, 128)], twin_s),
        (tw_hbm.at[:, pl.ds(group, 128)], tw_s),
        (tr_hbm.at[:, pl.ds(group, 128)], tr_s),
        (gain_hbm.at[:, pl.ds(col, 128)], gain_s),
        (gain_hbm.at[:, pl.ds(twin_col, 128)], twin_gain_s),
        (ihist_hbm, ihist_s),
        (step_hbm, step_s),
    )
    big = tuple(
        (saved_hbm.at[pl.ds(kv * 4 + c * 2, 2)], saved_s.at[p * 32 + kv * 2 : p * 32 + kv * 2 + 2])
        for p, c in enumerate((1 - core, core))
        for kv in range(16)
    )
    copies = fetch(small + big, sems)
    for copy in copies[: len(small)]:
        copy.wait()

    tin = tin_s[...].astype(f32)
    vec_ref[0:4, :] = tin
    vec_ref[4:8, :] = tw_s[...].astype(f32)
    vec_ref[8:12, :] = tr_s[...].astype(f32)
    place = lax.broadcasted_iota(jnp.int32, (1, 64), 1)
    first = lax.broadcasted_iota(jnp.int32, (1, 128), 1) < 64

    twin_head = (rank ^ 1) * 2

    def of_head(k, h):
        return jnp.sum(jnp.where(place == h, heads_s[k : k + 1], 0.0), axis=-1, keepdims=True)

    def spread(k, h):
        return jnp.where(first, of_head(k, h), of_head(k, h + 1))

    vec_ref[12:13, :] = -jnp.exp(spread(0, head))
    vec_ref[13:14, :] = spread(1, head)
    vec_ref[14:15, :] = spread(2, head)
    vec_ref[15:16, :] = gain_s[...]
    vec_ref[16:20, :] = twin_s[...].astype(f32)
    vec_ref[20:21, :] = -jnp.exp(spread(0, twin_head))
    vec_ref[21:22, :] = spread(1, twin_head)
    vec_ref[22:23, :] = spread(2, twin_head)
    vec_ref[23:24, :] = twin_gain_s[...]

    acc_row = acc_s[...]
    acc = jnp.broadcast_to(acc_row.astype(f32), (128, 64)).T
    acc_ref[...] = acc
    rows = [ihist_s[t].astype(f32) for t in range(7)]
    taps = [tin[k : k + 1] for k in range(4)]
    for i, part in enumerate(old_parts(taps, windows(rows, acc))):
        held_s[4 + i] = part

    def wide(pair):
        return jnp.concatenate([jnp.broadcast_to(v, (64, 64)) for v in pair], axis=0).T

    weights = [[], [], [], []]
    totals = []
    for h in range(2):
        rate = -jnp.exp(of_head(0, head + h))
        steps = [ls_s[t, h : h + 1, :] for t in range(4)]
        keep = [(acc_row > t).astype(f32) for t in range(4)]
        logs = [rate * steps[t] * keep[t] for t in range(4)]
        tail = jnp.zeros((1, 64), f32)
        for t in (3, 2, 1, 0):
            weights[t].append(keep[t] * jnp.exp(tail) * steps[t])
            tail = tail + logs[t]
        totals.append(jnp.exp(tail))
    held_s[7] = wide(totals)
    for t in range(4):
        held_s[t] = silu(sum(taps[k] * rows[t + k] for k in range(4))) * wide(weights[t])

    for q in range(2):
        start = (1 - core) * 2 + q
        block = slice(q * 16, (q + 1) * 16)
        for t in range(8):
            sent_ref[t, block] = held_s[t, pl.ds(start, 16, stride=4), :]
    held = pltpu.make_async_copy(held_s, held_hbm, sent.at[9])
    held.start()

    row = lax.broadcasted_iota(jnp.int32, (256, 64), 0)
    base = jnp.where(row < 128, head, twin_head)
    pick = lax.broadcasted_iota(jnp.int32, (256, 64), 1) == base + ((row >> 6) & 1)
    wide_s[...] = dot(pick.astype(f32).astype(bf16), step_s[...]).astype(bf16)
    out = [pltpu.make_async_copy(wide_s, wide_hbm, sent.at[8])]
    out[0].start()
    out.append(held)
    for k in range(8):
        block = slice(k * 8, (k + 1) * 8)
        for copy in copies[len(small) + k * 4 : len(small) + k * 4 + 4]:
            copy.wait()
        low_s[block] = saved_s[block].astype(bf16)
        dest = (give_hbm if k < 4 else keep_hbm).at[slice((k % 4) * 8, (k % 4 + 1) * 8)]
        out.append(pltpu.make_async_copy(low_s.at[block], dest, sent.at[k]))
        out[-1].start()
    for copy in out:
        copy.wait()


def group_kernel(p0_ref, p1_ref, p2_ref, p3_ref, acc_ref, vec_ref, wall_hbm, mix_hbm, wall_s, mix_s, hist_s, sems):
    member = device_rank() & 3
    for x, p in enumerate((p0_ref, p1_ref, p2_ref, p3_ref)):
        at = pl.multiple_of((member ^ x) * 32, 32)
        wall_s[pl.ds(at, 32), :] = p[0:32, :]
        wall_s[pl.ds(128 + at, 32), :] = p[32:64, :]
        for t in range(7):
            hist_s[t, pl.ds(at, 16), :] = p[64:80, t * 128 : (t + 1) * 128].astype(f32)
            hist_s[t, pl.ds(at + 16, 16), :] = p[64:80, (7 + t) * 128 : (8 + t) * 128].astype(f32)
    copy = pltpu.make_async_copy(wall_s, wall_hbm, sems.at[0])
    copy.start()
    both = [hist_s[t].T for t in range(7)]
    acc = acc_ref[...]
    acc2 = jnp.concatenate([acc, acc], axis=0)
    taps = [
        jnp.concatenate(
            [
                jnp.broadcast_to(vec_ref[4 + k : 5 + k, :], (64, 128)),
                jnp.broadcast_to(vec_ref[8 + k : 9 + k, :], (64, 128)),
            ],
            axis=0,
        )
        for k in range(4)
    ]
    for i, part in enumerate(old_parts(taps, windows(both, acc2))):
        mix_s[i] = part[0:64]
        mix_s[3 + i] = part[64:128]
    for t in range(4):
        w_old = silu(sum(vec_ref[4 + k : 5 + k, :] * both[t + k][0:64] for k in range(4)))
        mix_s[6 + t] = w_old.astype(bf16).astype(f32)
    last = pltpu.make_async_copy(mix_s, mix_hbm, sems.at[1])
    last.start()
    copy.wait()
    last.wait()


def state_kernel(
    saved_hbm, held_hbm, mix_hbm, after_hbm, base_hbm, saved_s, base_s, held_s, mix_s, sems, sent
):
    blocks = [slice(k * 8, (k + 1) * 8) for k in range(8)]
    copies = fetch(
        [(saved_hbm.at[k], saved_s.at[k]) for k in blocks]
        + [(held_hbm, held_s), (mix_hbm.at[6:10], mix_s)],
        sems,
    )
    copies[8].wait()
    copies[9].wait()
    tot = jnp.concatenate([held_s[7], held_s[7]], axis=0).T
    at = jnp.concatenate(
        [jnp.concatenate([held_s[2 * p], held_s[2 * p + 1]], axis=0).T for p in range(2)], axis=1
    ).astype(bf16)
    b = mix_s[...].reshape(256, 128).astype(bf16)
    lane = lax.broadcasted_iota(jnp.int32, (1, 256), 1) & 63
    out = []
    for k in range(8):
        copies[k].wait()
        for s in range(k * 8, (k + 1) * 8):
            mask = (lane == s).astype(f32).astype(bf16)
            base_s[s] = saved_s[s] * tot[:, s : s + 1] + dot(at * mask, b)
        copy = pltpu.make_async_copy(base_s.at[blocks[k]], base_hbm.at[blocks[k]], sent.at[k])
        copy.start()
        out.append(copy)
    for copy in out:
        copy.wait()


def rounded(v):
    return v.astype(bf16).astype(f32)


def main_kernel(
    mine_ref,
    norm_hbm,
    wall_hbm,
    step_hbm,
    inner_hbm,
    gate_hbm,
    held_hbm,
    mix_hbm,
    low_hbm,
    twin_low_hbm,
    own_hbm,
    twin_own_ref,
    twin_inner_ref,
    twin_gate_ref,
    got_ref,
    vec_ref,
    out_hbm,
    norm_s,
    wall_s,
    step_s,
    inner_s,
    gate_s,
    mix_s,
    held_s,
    low_s,
    proj_s,
    nrm_s,
    rows_s,
    read_s,
    car_s,
    out_s,
    sems,
    sent,
):
    copies = fetch(
        (
            (norm_hbm, norm_s),
            (wall_hbm, wall_s),
            (step_hbm, step_s),
            (inner_hbm, inner_s),
            (gate_hbm, gate_s),
            (mix_hbm, mix_s),
            (held_hbm, held_s),
            (low_hbm, low_s.at[0]),
            (twin_low_hbm, low_s.at[1]),
            (own_hbm, proj_s),
        ),
        sems,
    )
    core = lax.axis_index("tp")
    copies[0].wait()
    gain = norm_s[...]
    for k in range(8):
        x = mine_ref[2 * k : 2 * k + 2].astype(f32).reshape(16, 2048)
        scale = lax.rsqrt(jnp.mean(x * x, axis=-1, keepdims=True) + EPSILON)
        nrm_s[k * 16 : (k + 1) * 16, :] = (x * scale * gain).astype(bf16)
    normed = nrm_s[...]
    copies[1].wait()
    both = rounded(dot(normed, wall_s[...], NT))
    rows_s[2] = both[:, 0:128]
    rows_s[3] = both[:, 128:256]
    copies[2].wait()
    both = dot(normed, step_s[...], NT)
    rows_s[0] = both[:, 0:128]
    rows_s[1] = both[:, 128:256]
    rows_s[5] = rounded(dot(normed, twin_inner_ref[...]))
    rows_s[7] = rounded(dot(normed, twin_gate_ref[...]))
    copies[3].wait()
    rows_s[4] = rounded(dot(normed, inner_s[...]))
    copies[4].wait()
    rows_s[6] = rounded(dot(normed, gate_s[...]))

    def at_time(ref, t, k):
        return jnp.concatenate([ref[k, pl.ds(q * 4 + t, 16, stride=8), :] for q in range(2)], axis=0)

    def put(ref, t, k, value):
        for q in range(2):
            ref[k, pl.ds(q * 4 + t, 16, stride=8), :] = value[q * 16 : (q + 1) * 16]

    def chosen(ref, k):
        return jnp.concatenate(
            [ref[k, pl.ds(core * 2 + q, 16, stride=4), :] for q in range(2)], axis=0
        )

    def conv_new(new, parts, taps):
        out = []
        for i in range(4):
            v = taps[3] * new[i]
            for d in range(1, i + 1):
                v = v + taps[3 - d] * new[i - d]
            out.append(silu(v if i == 3 else v + parts[i]))
        return out

    def taps_of(first):
        return [vec_ref[first + k : first + k + 1, :] for k in range(4)]

    def mixing(k, base, taps):
        new = [at_time(rows_s, t, k) for t in range(4)]
        return [rounded(v) for v in conv_new(new, [chosen(mix_s, base + i) for i in range(3)], taps)]

    copies[5].wait()
    write = mixing(2, 0, taps_of(4))
    read = mixing(3, 3, taps_of(8))
    for t in range(4):
        put(read_s, t, 0, read[t])
    quarter = lax.broadcasted_iota(jnp.int32, (16, 128), 0) >> 2
    copies[7].wait()
    copies[8].wait()
    for g in range(8):
        r = read_s[0, g * 16 : (g + 1) * 16, :].astype(bf16)
        for p in range(2):
            full = dot(r, low_s[p, g * 4 : (g + 1) * 4].reshape(512, 128), NT)
            v = full[:, 0:128]
            for q in range(1, 4):
                v = jnp.where(quarter == q, full[:, q * 128 : (q + 1) * 128], v)
            car_s[p, g * 16 : (g + 1) * 16, :] = v

    def score(x, y):
        return jnp.sum(x * y, axis=-1, keepdims=True)

    scores = [[score(read[i], write[j]) for j in range(i + 1)] for i in range(4)]
    past = [chosen(mix_s, 6 + t) for t in range(4)]
    copies[6].wait()
    olds = [[score(read[i], past[t]) for t in range(4)] for i in range(4)]
    for p in range(2):
        if p == 0:
            held = [chosen(held_s, t) for t in range(4)]
            parts = [chosen(held_s, 4 + t) for t in range(3)]
            tot = chosen(held_s, 7)
        else:
            held = [got_ref[t] for t in range(4)]
            parts = [got_ref[4 + t] for t in range(3)]
            tot = got_ref[7]
        inner = conv_new(
            [at_time(rows_s, t, 4 + p) for t in range(4)], parts, taps_of(16 if p else 0)
        )
        first = 20 if p else 12
        rate, skip, bias = (vec_ref[first + k : first + k + 1, :] for k in range(3))
        steps = []
        for t in range(4):
            z = at_time(rows_s, t, p) + bias
            steps.append(jnp.maximum(z, 0.0) + jnp.log1p(jnp.exp(-jnp.abs(z))))
        sums = [rate * steps[0]]
        for t in range(1, 4):
            sums.append(sums[-1] + rate * steps[t])
        moved = [steps[t] * inner[t] for t in range(4)]
        for i in range(4):
            state = tot * at_time(car_s, i, p)
            for t in range(4):
                state = state + held[t] * olds[i][t]
            y = jnp.exp(sums[i]) * state + skip * inner[i] + scores[i][i] * moved[i]
            for j in range(i):
                y = y + scores[i][j] * jnp.exp(sums[i] - sums[j]) * moved[j]
            put(read_s, i, p, y * silu(at_time(rows_s, i, 6 + p)))

    lane = lax.broadcasted_iota(jnp.int32, (128, 128), 1)
    gated = [read_s[p] for p in range(2)]
    sq = jnp.sum(gated[0] * gated[0] + gated[1] * gated[1], axis=-1, keepdims=True)
    hi = rounded(sq)
    out_s[:, 2048:2176] = jnp.where(lane == 0, hi, jnp.where(lane == 1, sq - hi, 0.0)).astype(bf16)
    unscaled = [
        (gated[p] * vec_ref[15 + 8 * p : 16 + 8 * p, :]).astype(bf16) for p in range(2)
    ]
    copies[9].wait()
    out = []
    for k in range(4):
        cols = slice(k * 512, (k + 1) * 512)
        value = dot(unscaled[0], proj_s[:, cols]) + dot(unscaled[1], twin_own_ref[:, cols])
        out_s[:, cols] = value.astype(bf16)
        cols = slice(k * 512, 2176 if k == 3 else (k + 1) * 512)
        out.append(pltpu.make_async_copy(out_s.at[:, cols], out_hbm.at[:, cols], sent.at[k]))
        out[-1].start()
    for copy in out:
        copy.wait()


def sum_kernel(in_ref, out_ref):
    total = in_ref[0].astype(f32)
    for k in range(1, 16):
        total = total + in_ref[k].astype(f32)
    squares = jnp.sum(total[:, 2048:2176], axis=-1, keepdims=True)
    out_ref[...] = (total[:, 0:2048] * lax.rsqrt(squares / INNER + EPSILON)).astype(bf16)


def whole(memory_space=pltpu.VMEM):
    return pl.BlockSpec(memory_space=memory_space)


def swapped(value, axis):
    return lax.ppermute(value, axis, [(k, k ^ 1) for k in range(lax.axis_size(axis))])


def params(mib, **kw):
    return pltpu.CompilerParams(vmem_limit_bytes=mib << 20, **kw)


def body(
    tokens,
    norm_gain,
    gate_proj,
    inner_proj,
    write_proj,
    read_proj,
    step_proj,
    step_bias,
    decay_log,
    skip_gain,
    conv_inner,
    conv_write,
    conv_read,
    out_gain,
    out_proj,
    saved_state,
    inner_history,
    write_history,
    read_history,
    last_steps,
    accepted,
):
    def hbm(value):
        return pltpu.with_memory_space_constraint(value, pltpu.HBM)

    anywhere = whole(pl.ANY)
    dma = pltpu.SemaphoreType.DMA

    def shape(*dims, kind=f32):
        return jax.ShapeDtypeStruct(dims, kind)

    saved = saved_state.reshape(64, 128, 128)
    sent, pack = pl.pallas_call(
        begin_kernel,
        out_shape=[pltpu.HBM((16, 8, 2048), bf16), shape(80, 2048, kind=bf16)],
        in_specs=[anywhere] * 5,
        out_specs=[anywhere, whole()],
        scratch_shapes=[
            pltpu.VMEM((8, 2048), bf16),
            pltpu.VMEM((7, 32, 64), bf16),
            pltpu.VMEM((7, 32, 64), bf16),
            dma((5,)),
            dma((16,)),
        ],
        compiler_params=params(4),
        name="begin",
    )(
        hbm(tokens),
        hbm(write_proj.T),
        hbm(read_proj.T),
        hbm(write_history.transpose(1, 2, 0)),
        hbm(read_history.transpose(1, 2, 0)),
    )
    mine = lax.all_to_all(sent, "kv", 0, 0, tiled=True)
    pack_kv = swapped(pack, "kv")
    pack_tp = swapped(pack, "tp")
    pack_both = swapped(pack_kv, "tp")
    gate_other = swapped(gate_proj, "tp")
    inner_other = swapped(inner_proj, "tp")
    out_other = swapped(out_proj, "tp")

    keep, give, held, step, acc, vec, derived = pl.pallas_call(
        prep_kernel,
        in_specs=[anywhere] * 12,
        out_specs=[anywhere] * 4 + [whole()] * 3,
        out_shape=[
            pltpu.HBM((32, 128, 128), bf16),
            pltpu.HBM((32, 128, 128), bf16),
            pltpu.HBM((8, 64, 128), f32),
            pltpu.HBM((256, 2048), bf16),
            shape(64, 128),
            shape(24, 128),
            shape(8, 32, 128),
        ],
        scratch_shapes=[
            pltpu.VMEM((8, 64, 128), f32),
            pltpu.VMEM((64, 128, 128), bf16),
            pltpu.VMEM((256, 2048), bf16),
            pltpu.VMEM((64, 128, 128), f32),
            pltpu.VMEM((7, 64, 128), bf16),
            pltpu.VMEM((4, 128), bf16),
            pltpu.VMEM((4, 128), bf16),
            pltpu.VMEM((4, 128), bf16),
            pltpu.VMEM((4, 128), bf16),
            pltpu.VMEM((1, 128), f32),
            pltpu.VMEM((1, 128), f32),
            pltpu.VMEM((4, 2, 64), f32),
            pltpu.VMEM((1, 64), jnp.int32),
            pltpu.VMEM((3, 64), f32),
            pltpu.VMEM((64, 2048), bf16),
            dma((45,)),
            dma((10,)),
        ],
        compiler_params=params(12),
        name="prep",
    )(
        *[
            hbm(v)
            for v in (
                saved,
                inner_history.transpose(1, 0, 2),
                conv_inner,
                conv_write,
                conv_read,
                out_gain[None, :],
                last_steps.transpose(1, 2, 0),
                accepted[None, :],
                decay_log[None, :],
                skip_gain[None, :],
                step_bias[None, :],
                step_proj.T,
            )
        ]
    )
    wall, mix = pl.pallas_call(
        group_kernel,
        in_specs=[whole()] * 6,
        out_specs=[anywhere] * 2,
        out_shape=[pltpu.HBM((256, 2048), bf16), pltpu.HBM((10, 64, 128), f32)],
        scratch_shapes=[
            pltpu.VMEM((256, 2048), bf16),
            pltpu.VMEM((10, 64, 128), f32),
            pltpu.VMEM((7, 128, 128), f32),
            dma((2,)),
        ],
        compiler_params=params(6),
        name="group",
    )(pack, pack_tp, pack_kv, pack_both, acc, vec)

    low_twin = swapped(give, "tp")
    derived_twin = swapped(derived, "tp")
    partial = pl.pallas_call(
        main_kernel,
        in_specs=[whole()] + [anywhere] * 10 + [whole()] * 5,
        out_specs=anywhere,
        out_shape=pltpu.HBM((128, 2176), bf16),
        scratch_shapes=[
            pltpu.VMEM((1, 2048), f32),
            pltpu.VMEM((256, 2048), bf16),
            pltpu.VMEM((256, 2048), bf16),
            pltpu.VMEM((2048, 128), bf16),
            pltpu.VMEM((2048, 128), bf16),
            pltpu.VMEM((10, 64, 128), f32),
            pltpu.VMEM((8, 64, 128), f32),
            pltpu.VMEM((2, 32, 128, 128), bf16),
            pltpu.VMEM((128, 2048), bf16),
            pltpu.VMEM((128, 2048), bf16),
            pltpu.VMEM((8, 128, 128), f32),
            pltpu.VMEM((2, 128, 128), f32),
            pltpu.VMEM((2, 128, 128), f32),
            pltpu.VMEM((128, 2176), bf16),
            dma((10,)),
            dma((4,)),
        ],
        compiler_params=params(12),
        name="main",
    )(
        mine,
        *[
            hbm(v)
            for v in (
                norm_gain[None, :],
                wall,
                step,
                inner_proj,
                gate_proj,
                held,
                mix,
                keep,
                low_twin,
                out_proj,
            )
        ],
        out_other,
        inner_other,
        gate_other,
        derived_twin,
        vec,
    )
    arrived = lax.all_to_all(partial.reshape(16, 8, 2176), "kv", 0, 0, tiled=True)
    base = pl.pallas_call(
        state_kernel,
        in_specs=[anywhere] * 4,
        out_specs=anywhere,
        out_shape=shape(64, 128, 128),
        scratch_shapes=[
            pltpu.VMEM((64, 128, 128), f32),
            pltpu.VMEM((64, 128, 128), f32),
            pltpu.VMEM((8, 64, 128), f32),
            pltpu.VMEM((4, 64, 128), f32),
            dma((10,)),
            dma((8,)),
        ],
        compiler_params=params(12),
        name="state",
    )(hbm(saved), hbm(held), hbm(mix), hbm(partial))
    mixed = pl.pallas_call(
        sum_kernel,
        in_specs=[whole()],
        out_specs=whole(),
        out_shape=shape(8, 2048, kind=bf16),
        compiler_params=params(4),
        name="total",
    )(arrived)
    return mixed, base.reshape(64, 2, 64, 128)


def solution(mesh):
    both = ("kv", "tp")
    placed = (
        P(("dp", "kv", "tp"), None),
        P(),
        P(None, both),
        P(None, both),
        P(None, both),
        P(None, both),
        P(),
        P(),
        P(),
        P(),
        P(),
        P(),
        P(),
        P(),
        P(both, None),
        P("dp", both, None, None),
        P("dp", None, both),
        P("dp", None, both),
        P("dp", None, both),
        P("dp", None, both),
        P("dp"),
    )
    return jax.shard_map(
        body,
        mesh=mesh,
        in_specs=placed,
        out_specs=(P(("dp", "kv", "tp"), None), P("dp", both, None, None)),
        check_vma=False,
    )
```

```python
import jax
import jax.numpy as jnp
from jax import lax
from jax.experimental import pallas as pl
from jax.experimental.pallas import tpu as pltpu
from jax.sharding import PartitionSpec as P


EPSILON = 0.1
INNER = 4096
f32 = jnp.float32
bf16 = jnp.bfloat16
NT = (((1,), (1,)), ((), ()))
NN = (((1,), (0,)), ((), ()))


def dot(a, b, dims=NN):
    return lax.dot_general(a, b, dims, preferred_element_type=f32)


def silu(x):
    return x * (1.0 / (1.0 + jnp.exp(-x)))


def fetch(pairs, sems):
    copies = [pltpu.make_async_copy(src, dst, sems.at[k]) for k, (src, dst) in enumerate(pairs)]
    for copy in copies:
        copy.start()
    return copies


def device_rank():
    return lax.axis_index("kv") * 2 + lax.axis_index("tp")


def begin_kernel(
    tok_hbm, w_hbm, r_hbm, wh_hbm, rh_hbm, all_hbm, out_ref, tok_s, wh_s, rh_s, sems, sent
):
    copies = fetch(
        (
            (tok_hbm, tok_s),
            (wh_hbm, wh_s),
            (rh_hbm, rh_s),
            (w_hbm, out_ref.at[0:32]),
            (r_hbm, out_ref.at[32:64]),
        ),
        sems,
    )
    copies[0].wait()
    out = fetch([(tok_s, all_hbm.at[k]) for k in range(16)], sent)
    copies[1].wait()
    copies[2].wait()
    for t in range(7):
        both = jnp.concatenate([wh_s[t].astype(f32), rh_s[t].astype(f32)], axis=1).astype(bf16)
        out_ref[64:80, t * 128 : (t + 1) * 128] = both[0:16]
        out_ref[64:80, (7 + t) * 128 : (8 + t) * 128] = both[16:32]
    out_ref[64:80, 1792:2048] = jnp.zeros((16, 256), bf16)
    for copy in copies[3:] + out:
        copy.wait()


def windows(rows, acc):
    out = []
    for j in range(3):
        w = rows[j]
        for a in range(1, 5):
            w = jnp.where(acc == a, rows[a + j], w)
        out.append(w)
    return out


def old_parts(taps, w):
    return (
        taps[0] * w[0] + taps[1] * w[1] + taps[2] * w[2],
        taps[0] * w[1] + taps[1] * w[2],
        taps[0] * w[2],
    )


def prep_kernel(
    saved_hbm,
    ihist_hbm,
    tin_hbm,
    tw_hbm,
    tr_hbm,
    gain_hbm,
    ls_hbm,
    acc_hbm,
    decay_hbm,
    skip_hbm,
    bias_hbm,
    give_hbm,
    held_s,
    acc_ref,
    vec_ref,
    sent_ref,
    low_s,
    saved_s,
    ihist_s,
    tin_s,
    twin_s,
    tw_s,
    tr_s,
    gain_s,
    twin_gain_s,
    ls_s,
    acc_s,
    heads_s,
    sems,
    sent,
):
    rank = device_rank()
    core = rank & 1
    head = rank * 2
    col = pl.multiple_of(rank * 128, 128)
    twin_col = pl.multiple_of((rank ^ 1) * 128, 128)
    group = pl.multiple_of((rank >> 2) * 128, 128)
    small = (
        (acc_hbm, acc_s),
        (ls_hbm, ls_s),
        (decay_hbm, heads_s.at[0:1]),
        (skip_hbm, heads_s.at[1:2]),
        (bias_hbm, heads_s.at[2:3]),
        (tin_hbm.at[:, pl.ds(col, 128)], tin_s),
        (tin_hbm.at[:, pl.ds(twin_col, 128)], twin_s),
        (tw_hbm.at[:, pl.ds(group, 128)], tw_s),
        (tr_hbm.at[:, pl.ds(group, 128)], tr_s),
        (gain_hbm.at[:, pl.ds(col, 128)], gain_s),
        (gain_hbm.at[:, pl.ds(twin_col, 128)], twin_gain_s),
        (ihist_hbm, ihist_s),
    )
    big = tuple(
        (saved_hbm.at[pl.ds(kv * 4 + (1 - core) * 2, 2)], saved_s.at[kv * 2 : kv * 2 + 2])
        for kv in range(16)
    )
    copies = fetch(big + small, sems)
    out = []
    for k in range(4):
        block = slice(k * 8, (k + 1) * 8)
        for copy in copies[k * 4 : k * 4 + 4]:
            copy.wait()
        low_s[block] = saved_s[block].astype(bf16)
        out.append(pltpu.make_async_copy(low_s.at[block], give_hbm.at[block], sent.at[k]))
        out[-1].start()
    for copy in copies[len(big) :]:
        copy.wait()

    tin = tin_s[...].astype(f32)
    vec_ref[0:4, :] = tin
    vec_ref[4:8, :] = tw_s[...].astype(f32)
    vec_ref[8:12, :] = tr_s[...].astype(f32)
    place = lax.broadcasted_iota(jnp.int32, (1, 64), 1)
    first = lax.broadcasted_iota(jnp.int32, (1, 128), 1) < 64

    twin_head = (rank ^ 1) * 2

    def of_head(k, h):
        return jnp.sum(jnp.where(place == h, heads_s[k : k + 1], 0.0), axis=-1, keepdims=True)

    def spread(k, h):
        return jnp.where(first, of_head(k, h), of_head(k, h + 1))

    vec_ref[12:13, :] = -jnp.exp(spread(0, head))
    vec_ref[13:14, :] = spread(1, head)
    vec_ref[14:15, :] = spread(2, head)
    vec_ref[15:16, :] = gain_s[...]
    vec_ref[16:20, :] = twin_s[...].astype(f32)
    vec_ref[20:21, :] = -jnp.exp(spread(0, twin_head))
    vec_ref[21:22, :] = spread(1, twin_head)
    vec_ref[22:23, :] = spread(2, twin_head)
    vec_ref[23:24, :] = twin_gain_s[...]

    acc_row = acc_s[...]
    acc = jnp.broadcast_to(acc_row.astype(f32), (128, 64)).T
    acc_ref[...] = acc
    rows = [ihist_s[t].astype(f32) for t in range(7)]
    taps = [tin[k : k + 1] for k in range(4)]
    for i, part in enumerate(old_parts(taps, windows(rows, acc))):
        held_s[4 + i] = part

    def wide(pair):
        return jnp.concatenate([jnp.broadcast_to(v, (64, 64)) for v in pair], axis=0).T

    weights = [[], [], [], []]
    totals = []
    for h in range(2):
        rate = -jnp.exp(of_head(0, head + h))
        steps = [ls_s[t, h : h + 1, :] for t in range(4)]
        keep = [(acc_row > t).astype(f32) for t in range(4)]
        logs = [rate * steps[t] * keep[t] for t in range(4)]
        tail = jnp.zeros((1, 64), f32)
        for t in (3, 2, 1, 0):
            weights[t].append(keep[t] * jnp.exp(tail) * steps[t])
            tail = tail + logs[t]
        totals.append(jnp.exp(tail))
    held_s[7] = wide(totals)
    for t in range(4):
        held_s[t] = silu(sum(taps[k] * rows[t + k] for k in range(4))) * wide(weights[t])

    for q in range(2):
        start = (1 - core) * 2 + q
        block = slice(q * 16, (q + 1) * 16)
        for t in range(8):
            sent_ref[t, block] = held_s[t, pl.ds(start, 16, stride=4), :]
    for copy in out:
        copy.wait()


def group_kernel(p0_ref, p1_ref, p2_ref, p3_ref, acc_ref, vec_ref, wall_hbm, mix_hbm, wall_s, mix_s, hist_s, sems):
    member = device_rank() & 3
    for x, p in enumerate((p0_ref, p1_ref, p2_ref, p3_ref)):
        at = pl.multiple_of((member ^ x) * 32, 32)
        wall_s[pl.ds(at, 32), :] = p[0:32, :]
        wall_s[pl.ds(128 + at, 32), :] = p[32:64, :]
        for t in range(7):
            hist_s[t, pl.ds(at, 16), :] = p[64:80, t * 128 : (t + 1) * 128].astype(f32)
            hist_s[t, pl.ds(at + 16, 16), :] = p[64:80, (7 + t) * 128 : (8 + t) * 128].astype(f32)
    copy = pltpu.make_async_copy(wall_s, wall_hbm, sems.at[0])
    copy.start()
    both = [hist_s[t].T for t in range(7)]
    acc = acc_ref[...]
    acc2 = jnp.concatenate([acc, acc], axis=0)
    taps = [
        jnp.concatenate(
            [
                jnp.broadcast_to(vec_ref[4 + k : 5 + k, :], (64, 128)),
                jnp.broadcast_to(vec_ref[8 + k : 9 + k, :], (64, 128)),
            ],
            axis=0,
        )
        for k in range(4)
    ]
    for i, part in enumerate(old_parts(taps, windows(both, acc2))):
        mix_s[i] = part[0:64]
        mix_s[3 + i] = part[64:128]
    for t in range(4):
        w_old = silu(sum(vec_ref[4 + k : 5 + k, :] * both[t + k][0:64] for k in range(4)))
        mix_s[6 + t] = w_old.astype(bf16).astype(f32)
    last = pltpu.make_async_copy(mix_s, mix_hbm, sems.at[1])
    last.start()
    copy.wait()
    last.wait()


def state_kernel(
    saved_hbm, mix_hbm, after_hbm, held_s, base_hbm, saved_s, base_s, mix_s, sems, sent
):
    blocks = [slice(k * 8, (k + 1) * 8) for k in range(8)]
    copies = fetch(
        [(saved_hbm.at[k], saved_s.at[k]) for k in blocks]
        + [(mix_hbm.at[6:10], mix_s)],
        sems,
    )
    copies[8].wait()
    tot = jnp.concatenate([held_s[7], held_s[7]], axis=0).T
    at = jnp.concatenate(
        [jnp.concatenate([held_s[2 * p], held_s[2 * p + 1]], axis=0).T for p in range(2)], axis=1
    ).astype(bf16)
    b = mix_s[...].reshape(256, 128).astype(bf16)
    lane = lax.broadcasted_iota(jnp.int32, (1, 256), 1) & 63
    out = []
    for k in range(8):
        copies[k].wait()
        for s in range(k * 8, (k + 1) * 8):
            mask = (lane == s).astype(f32).astype(bf16)
            base_s[s] = saved_s[s] * tot[:, s : s + 1] + dot(at * mask, b)
        copy = pltpu.make_async_copy(base_s.at[blocks[k]], base_hbm.at[blocks[k]], sent.at[k])
        copy.start()
        out.append(copy)
    for copy in out:
        copy.wait()


def rounded(v):
    return v.astype(bf16).astype(f32)


def main_kernel(
    mine_ref,
    norm_hbm,
    wall_hbm,
    step_hbm,
    inner_hbm,
    gate_hbm,
    mix_hbm,
    saved_hbm,
    own_hbm,
    twin_own_hbm,
    got_hbm,
    held_s,
    twin_low_ref,
    twin_inner_ref,
    twin_gate_ref,
    vec_ref,
    out_hbm,
    norm_s,
    wall_s,
    step_s,
    inner_s,
    gate_s,
    mix_s,
    got_ref,
    low_s,
    proj_s,
    nrm_s,
    rows_s,
    read_s,
    part_s,
    out_s,
    sems,
    sent,
):
    core = lax.axis_index("tp")
    copies = fetch(
        (
            (norm_hbm, norm_s),
            (wall_hbm, wall_s),
            (step_hbm, step_s),
            (inner_hbm, inner_s),
            (gate_hbm, gate_s),
            (mix_hbm, mix_s),
            (got_hbm, got_ref),
            (own_hbm, proj_s.at[0]),
            (twin_own_hbm, proj_s.at[1]),
        )
        + tuple(
            (saved_hbm.at[pl.ds(kv * 4 + core * 2, 2)], low_s.at[kv * 2 : kv * 2 + 2])
            for kv in range(16)
        ),
        sems,
    )
    copies[0].wait()
    gain = norm_s[...]
    for k in range(8):
        x = mine_ref[2 * k : 2 * k + 2].astype(f32).reshape(16, 2048)
        scale = lax.rsqrt(jnp.mean(x * x, axis=-1, keepdims=True) + EPSILON)
        nrm_s[k * 16 : (k + 1) * 16, :] = (x * scale * gain).astype(bf16)
    normed = nrm_s[...]
    for copy in copies[1:5]:
        copy.wait()
    both = rounded(dot(normed, wall_s[...], NT))
    rows_s[2] = both[:, 0:128]
    rows_s[3] = both[:, 128:256]
    weights = [inner_s[...], twin_inner_ref[...], gate_s[...], twin_gate_ref[...]]
    both = rounded(dot(normed, jnp.concatenate(weights, axis=1)))
    for k in range(4):
        rows_s[4 + k] = both[:, k * 128 : (k + 1) * 128]
    both = dot(normed, step_s[...], NT)
    lane = lax.broadcasted_iota(jnp.int32, (64, 256), 1)
    head = (device_rank() ^ (lane >> 7)) * 2 + ((lane >> 6) & 1)
    pick = lax.broadcasted_iota(jnp.int32, (64, 256), 0) == head
    pick = pick.astype(f32).astype(bf16)
    high = both.astype(bf16)
    rest = both - high.astype(f32)
    mid = rest.astype(bf16)
    low = (rest - mid.astype(f32)).astype(bf16)
    both = dot(high, pick) + (dot(mid, pick) + dot(low, pick))
    rows_s[0] = both[:, 0:128]
    rows_s[1] = both[:, 128:256]
    for copy in copies[5:]:
        copy.wait()

    def at_time(ref, t, k):
        return jnp.concatenate([ref[k, pl.ds(q * 4 + t, 16, stride=8), :] for q in range(2)], axis=0)

    def put(ref, t, k, value):
        for q in range(2):
            ref[k, pl.ds(q * 4 + t, 16, stride=8), :] = value[q * 16 : (q + 1) * 16]

    def chosen(ref, k):
        return jnp.concatenate(
            [ref[k, pl.ds(core * 2 + q, 16, stride=4), :] for q in range(2)], axis=0
        )

    def conv_new(new, parts, taps):
        out = []
        for i in range(4):
            v = taps[3] * new[i]
            for d in range(1, i + 1):
                v = v + taps[3 - d] * new[i - d]
            out.append(silu(v if i == 3 else v + parts[i]))
        return out

    def taps_of(first):
        return [vec_ref[first + k : first + k + 1, :] for k in range(4)]

    def mixing(k, base, taps):
        new = [at_time(rows_s, t, k) for t in range(4)]
        return [rounded(v) for v in conv_new(new, [chosen(mix_s, base + i) for i in range(3)], taps)]

    write = mixing(2, 0, taps_of(4))
    read = mixing(3, 3, taps_of(8))
    for t in range(4):
        put(read_s, t, 0, read[t])

    def score(x, y):
        return jnp.sum(x * y, axis=-1, keepdims=True)

    scores = [[score(read[i], write[j]) for j in range(i + 1)] for i in range(4)]
    past = [chosen(mix_s, 6 + t) for t in range(4)]
    olds = [[score(read[i], past[t]) for t in range(4)] for i in range(4)]
    for p in range(2):
        if p == 0:
            held = [chosen(held_s, t) for t in range(4)]
            parts = [chosen(held_s, 4 + t) for t in range(3)]
            tot = chosen(held_s, 7)
        else:
            held = [got_ref[t] for t in range(4)]
            parts = [got_ref[4 + t] for t in range(3)]
            tot = got_ref[7]
        inner = conv_new(
            [at_time(rows_s, t, 4 + p) for t in range(4)], parts, taps_of(16 if p else 0)
        )
        first = 20 if p else 12
        rate, skip, bias = (vec_ref[first + k : first + k + 1, :] for k in range(3))
        steps = []
        for t in range(4):
            z = at_time(rows_s, t, p) + bias
            steps.append(jnp.maximum(z, 0.0) + jnp.log1p(jnp.exp(-jnp.abs(z))))
        sums = [rate * steps[0]]
        for t in range(1, 4):
            sums.append(sums[-1] + rate * steps[t])
        moved = [steps[t] * inner[t] for t in range(4)]
        for i in range(4):
            decay = jnp.exp(sums[i])
            state = held[0] * olds[i][0]
            for t in range(1, 4):
                state = state + held[t] * olds[i][t]
            y = decay * state + skip * inner[i] + scores[i][i] * moved[i]
            for j in range(i):
                y = y + scores[i][j] * jnp.exp(sums[i] - sums[j]) * moved[j]
            gate = silu(at_time(rows_s, i, 6 + p))
            put(part_s, i, p, y * gate)
            put(part_s, i, 2 + p, decay * tot * gate)

    quarter = lax.broadcasted_iota(jnp.int32, (16, 128), 0) >> 2
    for g in range(8):
        rows = slice(g * 16, (g + 1) * 16)
        r = read_s[0, rows, :].astype(bf16)
        for p, low in enumerate((low_s, twin_low_ref)):
            full = dot(r, low[g * 4 : (g + 1) * 4].reshape(512, 128).astype(bf16), NT)
            v = full[:, 0:128]
            for q in range(1, 4):
                v = jnp.where(quarter == q, full[:, q * 128 : (q + 1) * 128], v)
            part_s[p, rows, :] = part_s[p, rows, :] + part_s[2 + p, rows, :] * v

    lane = lax.broadcasted_iota(jnp.int32, (128, 128), 1)
    gated = [part_s[p] for p in range(2)]
    sq = jnp.sum(gated[0] * gated[0] + gated[1] * gated[1], axis=-1, keepdims=True)
    hi = rounded(sq)
    out_s[:, 2048:2176] = jnp.where(lane == 0, hi, jnp.where(lane == 1, sq - hi, 0.0)).astype(bf16)
    unscaled = [
        (gated[p] * vec_ref[15 + 8 * p : 16 + 8 * p, :]).astype(bf16) for p in range(2)
    ]
    out = []
    for k in range(4):
        cols = slice(k * 512, (k + 1) * 512)
        value = dot(unscaled[0], proj_s[0, :, cols]) + dot(unscaled[1], proj_s[1, :, cols])
        out_s[:, cols] = value.astype(bf16)
        cols = slice(k * 512, 2176 if k == 3 else (k + 1) * 512)
        out.append(pltpu.make_async_copy(out_s.at[:, cols], out_hbm.at[:, cols], sent.at[k]))
        out[-1].start()
    for copy in out:
        copy.wait()


def sum_kernel(in_ref, out_ref):
    total = in_ref[0].astype(f32)
    for k in range(1, 16):
        total = total + in_ref[k].astype(f32)
    squares = jnp.sum(total[:, 2048:2176], axis=-1, keepdims=True)
    out_ref[...] = (total[:, 0:2048] * lax.rsqrt(squares / INNER + EPSILON)).astype(bf16)


def whole(memory_space=pltpu.VMEM):
    return pl.BlockSpec(memory_space=memory_space)


def swapped(value, axis):
    return lax.ppermute(value, axis, [(k, k ^ 1) for k in range(lax.axis_size(axis))])


def params(mib, **kw):
    return pltpu.CompilerParams(vmem_limit_bytes=mib << 20, **kw)


def body(
    tokens,
    norm_gain,
    gate_proj,
    inner_proj,
    write_proj,
    read_proj,
    step_proj,
    step_bias,
    decay_log,
    skip_gain,
    conv_inner,
    conv_write,
    conv_read,
    out_gain,
    out_proj,
    saved_state,
    inner_history,
    write_history,
    read_history,
    last_steps,
    accepted,
):
    def hbm(value):
        return pltpu.with_memory_space_constraint(value, pltpu.HBM)

    anywhere = whole(pl.ANY)
    dma = pltpu.SemaphoreType.DMA

    def shape(*dims, kind=f32):
        return jax.ShapeDtypeStruct(dims, kind)

    saved = saved_state.reshape(64, 128, 128)
    sent, pack = pl.pallas_call(
        begin_kernel,
        out_shape=[pltpu.HBM((16, 8, 2048), bf16), shape(80, 2048, kind=bf16)],
        in_specs=[anywhere] * 5,
        out_specs=[anywhere, whole()],
        scratch_shapes=[
            pltpu.VMEM((8, 2048), bf16),
            pltpu.VMEM((7, 32, 64), bf16),
            pltpu.VMEM((7, 32, 64), bf16),
            dma((5,)),
            dma((16,)),
        ],
        compiler_params=params(4),
        name="begin",
    )(
        hbm(tokens),
        hbm(write_proj.T),
        hbm(read_proj.T),
        hbm(write_history.transpose(1, 2, 0)),
        hbm(read_history.transpose(1, 2, 0)),
    )
    mine = lax.all_to_all(sent, "kv", 0, 0, tiled=True)
    pack_kv = swapped(pack, "kv")
    pack_tp = swapped(pack, "tp")
    pack_both = swapped(pack_kv, "tp")
    gate_other = swapped(gate_proj, "tp")
    inner_other = swapped(inner_proj, "tp")
    out_other = swapped(out_proj, "tp")

    give, held, acc, vec, derived = pl.pallas_call(
        prep_kernel,
        in_specs=[anywhere] * 11,
        out_specs=[anywhere] + [whole()] * 4,
        out_shape=[
            pltpu.HBM((32, 128, 128), bf16),
            shape(8, 64, 128),
            shape(64, 128),
            shape(24, 128),
            shape(8, 32, 128),
        ],
        scratch_shapes=[
            pltpu.VMEM((32, 128, 128), bf16),
            pltpu.VMEM((32, 128, 128), f32),
            pltpu.VMEM((7, 64, 128), bf16),
            pltpu.VMEM((4, 128), bf16),
            pltpu.VMEM((4, 128), bf16),
            pltpu.VMEM((4, 128), bf16),
            pltpu.VMEM((4, 128), bf16),
            pltpu.VMEM((1, 128), f32),
            pltpu.VMEM((1, 128), f32),
            pltpu.VMEM((4, 2, 64), f32),
            pltpu.VMEM((1, 64), jnp.int32),
            pltpu.VMEM((3, 64), f32),
            dma((28,)),
            dma((4,)),
        ],
        compiler_params=params(12),
        name="prep",
    )(
        *[
            hbm(v)
            for v in (
                saved,
                inner_history.transpose(1, 0, 2),
                conv_inner,
                conv_write,
                conv_read,
                out_gain[None, :],
                last_steps.transpose(1, 2, 0),
                accepted[None, :],
                decay_log[None, :],
                skip_gain[None, :],
                step_bias[None, :],
            )
        ]
    )
    wall, mix = pl.pallas_call(
        group_kernel,
        in_specs=[whole()] * 6,
        out_specs=[anywhere] * 2,
        out_shape=[pltpu.HBM((256, 2048), bf16), pltpu.HBM((10, 64, 128), f32)],
        scratch_shapes=[
            pltpu.VMEM((256, 2048), bf16),
            pltpu.VMEM((10, 64, 128), f32),
            pltpu.VMEM((7, 128, 128), f32),
            dma((2,)),
        ],
        compiler_params=params(6),
        name="group",
    )(pack, pack_tp, pack_kv, pack_both, acc, vec)

    derived_twin = swapped(derived, "tp")
    low_twin = swapped(give, "tp")
    partial = pl.pallas_call(
        main_kernel,
        in_specs=[whole()] + [anywhere] * 10 + [whole()] * 5,
        out_specs=anywhere,
        out_shape=pltpu.HBM((128, 2176), bf16),
        scratch_shapes=[
            pltpu.VMEM((1, 2048), f32),
            pltpu.VMEM((256, 2048), bf16),
            pltpu.VMEM((64, 2048), bf16),
            pltpu.VMEM((2048, 128), bf16),
            pltpu.VMEM((2048, 128), bf16),
            pltpu.VMEM((10, 64, 128), f32),
            pltpu.VMEM((8, 32, 128), f32),
            pltpu.VMEM((32, 128, 128), f32),
            pltpu.VMEM((2, 128, 2048), bf16),
            pltpu.VMEM((128, 2048), bf16),
            pltpu.VMEM((8, 128, 128), f32),
            pltpu.VMEM((1, 128, 128), f32),
            pltpu.VMEM((4, 128, 128), f32),
            pltpu.VMEM((128, 2176), bf16),
            dma((25,)),
            dma((4,)),
        ],
        compiler_params=params(12),
        name="main",
    )(
        mine,
        *[
            hbm(v)
            for v in (
                norm_gain[None, :],
                wall,
                step_proj.T,
                inner_proj,
                gate_proj,
                mix,
                saved,
                out_proj,
                out_other,
                derived_twin,
            )
        ],
        held,
        low_twin,
        inner_other,
        gate_other,
        vec,
    )
    arrived = lax.all_to_all(partial.reshape(16, 8, 2176), "kv", 0, 0, tiled=True)
    base = pl.pallas_call(
        state_kernel,
        in_specs=[anywhere] * 3 + [whole()],
        out_specs=anywhere,
        out_shape=shape(64, 128, 128),
        scratch_shapes=[
            pltpu.VMEM((64, 128, 128), f32),
            pltpu.VMEM((64, 128, 128), f32),
            pltpu.VMEM((4, 64, 128), f32),
            dma((9,)),
            dma((8,)),
        ],
        compiler_params=params(12),
        name="state",
    )(hbm(saved), hbm(mix), hbm(partial), held)
    mixed = pl.pallas_call(
        sum_kernel,
        in_specs=[whole()],
        out_specs=whole(),
        out_shape=shape(8, 2048, kind=bf16),
        compiler_params=params(4),
        name="total",
    )(arrived)
    return mixed, base.reshape(64, 2, 64, 128)


def solution(mesh):
    both = ("kv", "tp")
    placed = (
        P(("dp", "kv", "tp"), None),
        P(),
        P(None, both),
        P(None, both),
        P(None, both),
        P(None, both),
        P(),
        P(),
        P(),
        P(),
        P(),
        P(),
        P(),
        P(),
        P(both, None),
        P("dp", both, None, None),
        P("dp", None, both),
        P("dp", None, both),
        P("dp", None, both),
        P("dp", None, both),
        P("dp"),
    )
    return jax.shard_map(
        body,
        mesh=mesh,
        in_specs=placed,
        out_specs=(P(("dp", "kv", "tp"), None), P("dp", both, None, None)),
        check_vma=False,
    )
```

```python
import jax
import jax.numpy as jnp
from jax import lax
from jax.experimental import pallas as pl
from jax.experimental.pallas import tpu as pltpu
from jax.sharding import PartitionSpec as P


EPSILON = 0.1
INNER = 4096
f32 = jnp.float32
bf16 = jnp.bfloat16
NT = (((1,), (1,)), ((), ()))
NN = (((1,), (0,)), ((), ()))


def dot(a, b, dims=NN):
    return lax.dot_general(a, b, dims, preferred_element_type=f32)


def silu(x):
    return x * (1.0 / (1.0 + jnp.exp(-x)))


def fetch(pairs, sems):
    copies = [pltpu.make_async_copy(src, dst, sems.at[k]) for k, (src, dst) in enumerate(pairs)]
    for copy in copies:
        copy.start()
    return copies


def device_rank():
    return lax.axis_index("kv") * 2 + lax.axis_index("tp")


def begin_kernel(
    tok_hbm, w_hbm, r_hbm, wh_hbm, rh_hbm, all_hbm, out_ref, hist_ref, tok_s, wh_s, rh_s, sems, sent
):
    copies = fetch(
        (
            (tok_hbm, tok_s),
            (wh_hbm, wh_s),
            (rh_hbm, rh_s),
            (w_hbm, out_ref.at[0:32]),
            (r_hbm, out_ref.at[32:64]),
        ),
        sems,
    )
    copies[0].wait()
    out = fetch([(tok_s, all_hbm.at[k]) for k in range(16)], sent)
    copies[1].wait()
    copies[2].wait()
    for t in range(7):
        both = jnp.concatenate([wh_s[t].astype(f32), rh_s[t].astype(f32)], axis=1).astype(bf16)
        out_ref[64:80, t * 128 : (t + 1) * 128] = both[0:16]
        out_ref[64:80, (7 + t) * 128 : (8 + t) * 128] = both[16:32]
    out_ref[64:80, 1792:2048] = jnp.zeros((16, 256), bf16)
    hist_ref[...] = out_ref[64:80, :]
    for copy in copies[3:] + out:
        copy.wait()


def windows(rows, acc):
    out = []
    for j in range(3):
        w = rows[j]
        for a in range(1, 5):
            w = jnp.where(acc == a, rows[a + j], w)
        out.append(w)
    return out


def old_parts(taps, w):
    return (
        taps[0] * w[0] + taps[1] * w[1] + taps[2] * w[2],
        taps[0] * w[1] + taps[1] * w[2],
        taps[0] * w[2],
    )


def prep_kernel(
    saved_hbm,
    ihist_hbm,
    tin_hbm,
    tw_hbm,
    tr_hbm,
    gain_hbm,
    ls_hbm,
    acc_hbm,
    decay_hbm,
    skip_hbm,
    bias_hbm,
    give_hbm,
    held_s,
    acc_ref,
    vec_ref,
    sent_ref,
    low_s,
    saved_s,
    ihist_s,
    tin_s,
    twin_s,
    tw_s,
    tr_s,
    gain_s,
    twin_gain_s,
    ls_s,
    acc_s,
    heads_s,
    sems,
    sent,
):
    rank = device_rank()
    core = rank & 1
    head = rank * 2
    col = pl.multiple_of(rank * 128, 128)
    twin_col = pl.multiple_of((rank ^ 1) * 128, 128)
    group = pl.multiple_of((rank >> 2) * 128, 128)
    small = (
        (acc_hbm, acc_s),
        (ls_hbm, ls_s),
        (decay_hbm, heads_s.at[0:1]),
        (skip_hbm, heads_s.at[1:2]),
        (bias_hbm, heads_s.at[2:3]),
        (tin_hbm.at[:, pl.ds(col, 128)], tin_s),
        (tin_hbm.at[:, pl.ds(twin_col, 128)], twin_s),
        (tw_hbm.at[:, pl.ds(group, 128)], tw_s),
        (tr_hbm.at[:, pl.ds(group, 128)], tr_s),
        (gain_hbm.at[:, pl.ds(col, 128)], gain_s),
        (gain_hbm.at[:, pl.ds(twin_col, 128)], twin_gain_s),
        (ihist_hbm, ihist_s),
    )
    big = tuple(
        (saved_hbm.at[pl.ds(kv * 4 + (1 - core) * 2, 2)], saved_s.at[kv * 2 : kv * 2 + 2])
        for kv in range(16)
    )
    copies = fetch(big + small, sems)
    out = []
    for k in range(4):
        block = slice(k * 8, (k + 1) * 8)
        for copy in copies[k * 4 : k * 4 + 4]:
            copy.wait()
        low_s[block] = saved_s[block].astype(bf16)
        out.append(pltpu.make_async_copy(low_s.at[block], give_hbm.at[block], sent.at[k]))
        out[-1].start()
    for copy in copies[len(big) :]:
        copy.wait()

    tin = tin_s[...].astype(f32)
    vec_ref[0:4, :] = tin
    vec_ref[4:8, :] = tw_s[...].astype(f32)
    vec_ref[8:12, :] = tr_s[...].astype(f32)
    place = lax.broadcasted_iota(jnp.int32, (1, 64), 1)
    first = lax.broadcasted_iota(jnp.int32, (1, 128), 1) < 64

    twin_head = (rank ^ 1) * 2

    def of_head(k, h):
        return jnp.sum(jnp.where(place == h, heads_s[k : k + 1], 0.0), axis=-1, keepdims=True)

    def spread(k, h):
        return jnp.where(first, of_head(k, h), of_head(k, h + 1))

    vec_ref[12:13, :] = -jnp.exp(spread(0, head))
    vec_ref[13:14, :] = spread(1, head)
    vec_ref[14:15, :] = spread(2, head)
    vec_ref[15:16, :] = gain_s[...]
    vec_ref[16:20, :] = twin_s[...].astype(f32)
    vec_ref[20:21, :] = -jnp.exp(spread(0, twin_head))
    vec_ref[21:22, :] = spread(1, twin_head)
    vec_ref[22:23, :] = spread(2, twin_head)
    vec_ref[23:24, :] = twin_gain_s[...]

    acc_row = acc_s[...]
    acc = jnp.broadcast_to(acc_row.astype(f32), (128, 64)).T
    acc_ref[...] = acc
    rows = [ihist_s[t].astype(f32) for t in range(7)]
    taps = [tin[k : k + 1] for k in range(4)]
    for i, part in enumerate(old_parts(taps, windows(rows, acc))):
        held_s[4 + i] = part

    def wide(pair):
        return jnp.concatenate([jnp.broadcast_to(v, (64, 64)) for v in pair], axis=0).T

    weights = [[], [], [], []]
    totals = []
    for h in range(2):
        rate = -jnp.exp(of_head(0, head + h))
        steps = [ls_s[t, h : h + 1, :] for t in range(4)]
        keep = [(acc_row > t).astype(f32) for t in range(4)]
        logs = [rate * steps[t] * keep[t] for t in range(4)]
        tail = jnp.zeros((1, 64), f32)
        for t in (3, 2, 1, 0):
            weights[t].append(keep[t] * jnp.exp(tail) * steps[t])
            tail = tail + logs[t]
        totals.append(jnp.exp(tail))
    held_s[7] = wide(totals)
    for t in range(4):
        held_s[t] = silu(sum(taps[k] * rows[t + k] for k in range(4))) * wide(weights[t])

    for q in range(2):
        start = (1 - core) * 2 + q
        block = slice(q * 16, (q + 1) * 16)
        for t in range(8):
            sent_ref[t, block] = held_s[t, pl.ds(start, 16, stride=4), :]
    for copy in out:
        copy.wait()


def group_kernel(own_ref, twin_ref, near_ref, far_ref, acc_ref, vec_ref, mix_s, hist_s):
    member = device_rank() & 3
    pieces = (own_ref.at[64:80], twin_ref.at[64:80], near_ref, far_ref)
    for x, p in enumerate(pieces):
        at = pl.multiple_of((member ^ x) * 32, 32)
        for t in range(7):
            hist_s[t, pl.ds(at, 16), :] = p[:, t * 128 : (t + 1) * 128].astype(f32)
            hist_s[t, pl.ds(at + 16, 16), :] = p[:, (7 + t) * 128 : (8 + t) * 128].astype(f32)
    both = [hist_s[t].T for t in range(7)]
    acc = acc_ref[...]
    acc2 = jnp.concatenate([acc, acc], axis=0)
    taps = [
        jnp.concatenate(
            [
                jnp.broadcast_to(vec_ref[4 + k : 5 + k, :], (64, 128)),
                jnp.broadcast_to(vec_ref[8 + k : 9 + k, :], (64, 128)),
            ],
            axis=0,
        )
        for k in range(4)
    ]
    for i, part in enumerate(old_parts(taps, windows(both, acc2))):
        mix_s[i] = part[0:64]
        mix_s[3 + i] = part[64:128]
    for t in range(4):
        w_old = silu(sum(vec_ref[4 + k : 5 + k, :] * both[t + k][0:64] for k in range(4)))
        mix_s[6 + t] = w_old.astype(bf16).astype(f32)


def state_kernel(
    saved_hbm, after_hbm, held_s, mix_s, base_hbm, saved_s, base_s, sems, sent
):
    blocks = [slice(k * 8, (k + 1) * 8) for k in range(8)]
    copies = fetch([(saved_hbm.at[k], saved_s.at[k]) for k in blocks], sems)
    tot = jnp.concatenate([held_s[7], held_s[7]], axis=0).T
    at = jnp.concatenate(
        [jnp.concatenate([held_s[2 * p], held_s[2 * p + 1]], axis=0).T for p in range(2)], axis=1
    ).astype(bf16)
    b = mix_s[6:10].reshape(256, 128).astype(bf16)
    lane = lax.broadcasted_iota(jnp.int32, (1, 256), 1) & 63
    out = []
    for k in range(8):
        copies[k].wait()
        for first in range(k * 8, (k + 1) * 8, 4):
            parts = [at * (lane == first + q).astype(f32).astype(bf16) for q in range(4)]
            new = dot(jnp.concatenate(parts, axis=0), b)
            for q in range(4):
                s = first + q
                base_s[s] = saved_s[s] * tot[:, s : s + 1] + new[q * 128 : (q + 1) * 128]
        copy = pltpu.make_async_copy(base_s.at[blocks[k]], base_hbm.at[blocks[k]], sent.at[k])
        copy.start()
        out.append(copy)
    for copy in out:
        copy.wait()


def rounded(v):
    return v.astype(bf16).astype(f32)


def norm_kernel(mine_ref, norm_ref, own_ref, twin_ref, nrm_ref, rows_ref, wall_s):
    core = lax.axis_index("tp")
    for c, p in ((core, own_ref), (1 - core, twin_ref)):
        at = pl.multiple_of(c * 32, 32)
        wall_s[pl.ds(at, 32), :] = p[0:32, :]
        wall_s[pl.ds(64 + at, 32), :] = p[32:64, :]
    gain = norm_ref[...]
    for k in range(8):
        x = mine_ref[2 * k : 2 * k + 2].astype(f32).reshape(16, 2048)
        scale = lax.rsqrt(jnp.mean(x * x, axis=-1, keepdims=True) + EPSILON)
        nrm_ref[k * 16 : (k + 1) * 16, :] = (x * scale * gain).astype(bf16)
    rows_ref[...] = dot(nrm_ref[...], wall_s[...], NT).astype(bf16)


def rows_kernel(
    nrm_ref,
    step_hbm,
    inner_hbm,
    gate_hbm,
    twin_inner_hbm,
    twin_gate_hbm,
    own_hbm,
    twin_own_hbm,
    saved_hbm,
    rows_ref,
    proj_ref,
    low_ref,
    step_s,
    inner_s,
    gate_s,
    twin_inner_s,
    twin_gate_s,
    low_s,
    sems,
):
    core = lax.axis_index("tp")
    copies = fetch(
        (
            (step_hbm, step_s),
            (inner_hbm, inner_s),
            (gate_hbm, gate_s),
            (twin_inner_hbm, twin_inner_s),
            (twin_gate_hbm, twin_gate_s),
            (own_hbm, proj_ref.at[0]),
            (twin_own_hbm, proj_ref.at[1]),
        )
        + tuple(
            (saved_hbm.at[pl.ds(kv * 4 + core * 2, 2)], low_s.at[kv * 2 : kv * 2 + 2])
            for kv in range(16)
        ),
        sems,
    )
    normed = nrm_ref[...]
    for copy in copies[0:5]:
        copy.wait()
    weights = [inner_s[...], twin_inner_s[...], gate_s[...], twin_gate_s[...]]
    both = rounded(dot(normed, jnp.concatenate(weights, axis=1)))
    for k in range(4):
        rows_ref[2 + k] = both[:, k * 128 : (k + 1) * 128]
    both = dot(normed, step_s[...], NT)
    lane = lax.broadcasted_iota(jnp.int32, (64, 256), 1)
    head = (device_rank() ^ (lane >> 7)) * 2 + ((lane >> 6) & 1)
    pick = lax.broadcasted_iota(jnp.int32, (64, 256), 0) == head
    pick = pick.astype(f32).astype(bf16)
    high = both.astype(bf16)
    rest = both - high.astype(f32)
    mid = rest.astype(bf16)
    low = (rest - mid.astype(f32)).astype(bf16)
    both = dot(high, pick) + (dot(mid, pick) + dot(low, pick))
    rows_ref[0] = both[:, 0:128]
    rows_ref[1] = both[:, 128:256]
    for copy in copies[5:]:
        copy.wait()
    low_ref[...] = low_s[...].astype(bf16)


def main_kernel(
    own_rows_ref,
    near_rows_ref,
    rows_s,
    mix_s,
    got_ref,
    proj_s,
    low_s,
    held_s,
    twin_low_ref,
    vec_ref,
    out_hbm,
    pair_s,
    read_s,
    part_s,
    out_s,
    sent,
):
    core = lax.axis_index("tp")
    lower = (lax.axis_index("kv") & 1) == 0
    half = lax.broadcasted_iota(jnp.int32, (128, 128), 1) < 64
    own = own_rows_ref[...].astype(f32)
    near = near_rows_ref[...].astype(f32)
    left = jnp.where(lower, own, near)
    right = jnp.where(lower, near, own)
    pair_s[0] = jnp.where(half, left, pltpu.roll(right, 64, 1))
    pair_s[1] = jnp.where(half, pltpu.roll(left, 64, 1), right)

    def at_time(ref, t, k):
        return jnp.concatenate([ref[k, pl.ds(q * 4 + t, 16, stride=8), :] for q in range(2)], axis=0)

    def put(ref, t, k, value):
        for q in range(2):
            ref[k, pl.ds(q * 4 + t, 16, stride=8), :] = value[q * 16 : (q + 1) * 16]

    def chosen(ref, k):
        return jnp.concatenate(
            [ref[k, pl.ds(core * 2 + q, 16, stride=4), :] for q in range(2)], axis=0
        )

    def conv_new(new, parts, taps):
        out = []
        for i in range(4):
            v = taps[3] * new[i]
            for d in range(1, i + 1):
                v = v + taps[3 - d] * new[i - d]
            out.append(silu(v if i == 3 else v + parts[i]))
        return out

    def taps_of(first):
        return [vec_ref[first + k : first + k + 1, :] for k in range(4)]

    def mixing(k, base, taps):
        new = [at_time(pair_s, t, k) for t in range(4)]
        return [rounded(v) for v in conv_new(new, [chosen(mix_s, base + i) for i in range(3)], taps)]

    write = mixing(0, 0, taps_of(4))
    read = mixing(1, 3, taps_of(8))
    for t in range(4):
        put(read_s, t, 0, read[t])

    def score(x, y):
        return jnp.sum(x * y, axis=-1, keepdims=True)

    scores = [[score(read[i], write[j]) for j in range(i + 1)] for i in range(4)]
    past = [chosen(mix_s, 6 + t) for t in range(4)]
    olds = [[score(read[i], past[t]) for t in range(4)] for i in range(4)]
    for p in range(2):
        if p == 0:
            held = [chosen(held_s, t) for t in range(4)]
            parts = [chosen(held_s, 4 + t) for t in range(3)]
            tot = chosen(held_s, 7)
        else:
            held = [got_ref[t] for t in range(4)]
            parts = [got_ref[4 + t] for t in range(3)]
            tot = got_ref[7]
        inner = conv_new(
            [at_time(rows_s, t, 2 + p) for t in range(4)], parts, taps_of(16 if p else 0)
        )
        first = 20 if p else 12
        rate, skip, bias = (vec_ref[first + k : first + k + 1, :] for k in range(3))
        steps = []
        for t in range(4):
            z = at_time(rows_s, t, p) + bias
            steps.append(jnp.maximum(z, 0.0) + jnp.log1p(jnp.exp(-jnp.abs(z))))
        sums = [rate * steps[0]]
        for t in range(1, 4):
            sums.append(sums[-1] + rate * steps[t])
        moved = [steps[t] * inner[t] for t in range(4)]
        for i in range(4):
            decay = jnp.exp(sums[i])
            state = held[0] * olds[i][0]
            for t in range(1, 4):
                state = state + held[t] * olds[i][t]
            y = decay * state + skip * inner[i] + scores[i][i] * moved[i]
            for j in range(i):
                y = y + scores[i][j] * jnp.exp(sums[i] - sums[j]) * moved[j]
            gate = silu(at_time(rows_s, i, 4 + p))
            put(part_s, i, p, y * gate)
            put(part_s, i, 2 + p, decay * tot * gate)

    quarter = lax.broadcasted_iota(jnp.int32, (16, 128), 0) >> 2
    for g in range(8):
        rows = slice(g * 16, (g + 1) * 16)
        r = read_s[0, rows, :].astype(bf16)
        for p, low in enumerate((low_s, twin_low_ref)):
            full = dot(r, low[g * 4 : (g + 1) * 4].reshape(512, 128), NT)
            v = full[:, 0:128]
            for q in range(1, 4):
                v = jnp.where(quarter == q, full[:, q * 128 : (q + 1) * 128], v)
            part_s[p, rows, :] = part_s[p, rows, :] + part_s[2 + p, rows, :] * v

    lane = lax.broadcasted_iota(jnp.int32, (128, 128), 1)
    gated = [part_s[p] for p in range(2)]
    sq = jnp.sum(gated[0] * gated[0] + gated[1] * gated[1], axis=-1, keepdims=True)
    hi = rounded(sq)
    out_s[:, 2048:2176] = jnp.where(lane == 0, hi, jnp.where(lane == 1, sq - hi, 0.0)).astype(bf16)
    unscaled = [
        (gated[p] * vec_ref[15 + 8 * p : 16 + 8 * p, :]).astype(bf16) for p in range(2)
    ]
    out = []
    for k in range(4):
        cols = slice(k * 512, (k + 1) * 512)
        value = dot(unscaled[0], proj_s[0, :, cols]) + dot(unscaled[1], proj_s[1, :, cols])
        out_s[:, cols] = value.astype(bf16)
        cols = slice(k * 512, 2176 if k == 3 else (k + 1) * 512)
        out.append(pltpu.make_async_copy(out_s.at[:, cols], out_hbm.at[:, cols], sent.at[k]))
        out[-1].start()
    for copy in out:
        copy.wait()


def sum_kernel(in_ref, out_ref):
    total = in_ref[0].astype(f32)
    for k in range(1, 16):
        total = total + in_ref[k].astype(f32)
    squares = jnp.sum(total[:, 2048:2176], axis=-1, keepdims=True)
    out_ref[...] = (total[:, 0:2048] * lax.rsqrt(squares / INNER + EPSILON)).astype(bf16)


def whole(memory_space=pltpu.VMEM):
    return pl.BlockSpec(memory_space=memory_space)


def swapped(value, axis):
    return lax.ppermute(value, axis, [(k, k ^ 1) for k in range(lax.axis_size(axis))])


def params(mib, **kw):
    return pltpu.CompilerParams(vmem_limit_bytes=mib << 20, **kw)


def body(
    tokens,
    norm_gain,
    gate_proj,
    inner_proj,
    write_proj,
    read_proj,
    step_proj,
    step_bias,
    decay_log,
    skip_gain,
    conv_inner,
    conv_write,
    conv_read,
    out_gain,
    out_proj,
    saved_state,
    inner_history,
    write_history,
    read_history,
    last_steps,
    accepted,
):
    def hbm(value):
        return pltpu.with_memory_space_constraint(value, pltpu.HBM)

    anywhere = whole(pl.ANY)
    dma = pltpu.SemaphoreType.DMA

    def shape(*dims, kind=f32):
        return jax.ShapeDtypeStruct(dims, kind)

    saved = saved_state.reshape(64, 128, 128)
    sent, pack, hist = pl.pallas_call(
        begin_kernel,
        out_shape=[
            pltpu.HBM((16, 8, 2048), bf16),
            shape(80, 2048, kind=bf16),
            shape(16, 2048, kind=bf16),
        ],
        in_specs=[anywhere] * 5,
        out_specs=[anywhere, whole(), whole()],
        scratch_shapes=[
            pltpu.VMEM((8, 2048), bf16),
            pltpu.VMEM((7, 32, 64), bf16),
            pltpu.VMEM((7, 32, 64), bf16),
            dma((5,)),
            dma((16,)),
        ],
        compiler_params=params(4),
        name="begin",
    )(
        hbm(tokens),
        hbm(write_proj.T),
        hbm(read_proj.T),
        hbm(write_history.transpose(1, 2, 0)),
        hbm(read_history.transpose(1, 2, 0)),
    )
    mine = lax.all_to_all(sent, "kv", 0, 0, tiled=True)
    hist_kv = swapped(hist, "kv")
    pack_tp = swapped(pack, "tp")
    hist_both = swapped(hist_kv, "tp")
    gate_other = swapped(gate_proj, "tp")
    inner_other = swapped(inner_proj, "tp")
    out_other = swapped(out_proj, "tp")

    give, held, acc, vec, derived = pl.pallas_call(
        prep_kernel,
        in_specs=[anywhere] * 11,
        out_specs=[anywhere] + [whole()] * 4,
        out_shape=[
            pltpu.HBM((32, 128, 128), bf16),
            shape(8, 64, 128),
            shape(64, 128),
            shape(24, 128),
            shape(8, 32, 128),
        ],
        scratch_shapes=[
            pltpu.VMEM((32, 128, 128), bf16),
            pltpu.VMEM((32, 128, 128), f32),
            pltpu.VMEM((7, 64, 128), bf16),
            pltpu.VMEM((4, 128), bf16),
            pltpu.VMEM((4, 128), bf16),
            pltpu.VMEM((4, 128), bf16),
            pltpu.VMEM((4, 128), bf16),
            pltpu.VMEM((1, 128), f32),
            pltpu.VMEM((1, 128), f32),
            pltpu.VMEM((4, 2, 64), f32),
            pltpu.VMEM((1, 64), jnp.int32),
            pltpu.VMEM((3, 64), f32),
            dma((28,)),
            dma((4,)),
        ],
        compiler_params=params(12),
        name="prep",
    )(
        *[
            hbm(v)
            for v in (
                saved,
                inner_history.transpose(1, 0, 2),
                conv_inner,
                conv_write,
                conv_read,
                out_gain[None, :],
                last_steps.transpose(1, 2, 0),
                accepted[None, :],
                decay_log[None, :],
                skip_gain[None, :],
                step_bias[None, :],
            )
        ]
    )
    mix = pl.pallas_call(
        group_kernel,
        in_specs=[whole()] * 6,
        out_specs=whole(),
        out_shape=shape(10, 64, 128),
        scratch_shapes=[pltpu.VMEM((7, 128, 128), f32)],
        compiler_params=params(6),
        name="group",
    )(pack, pack_tp, hist_kv, hist_both, acc, vec)

    derived_twin = swapped(derived, "tp")
    low_twin = swapped(give, "tp")
    normed, own_rows = pl.pallas_call(
        norm_kernel,
        in_specs=[whole()] * 4,
        out_specs=[whole()] * 2,
        out_shape=[shape(128, 2048, kind=bf16), shape(128, 128, kind=bf16)],
        scratch_shapes=[pltpu.VMEM((128, 2048), bf16)],
        compiler_params=params(6),
        name="norm",
    )(mine, norm_gain[None, :], pack, pack_tp)
    near_rows = swapped(own_rows, "kv")
    rows, proj_v, low_v = pl.pallas_call(
        rows_kernel,
        in_specs=[whole()] + [anywhere] * 8,
        out_specs=[whole()] * 3,
        out_shape=[
            shape(6, 128, 128),
            shape(2, 128, 2048, kind=bf16),
            shape(32, 128, 128, kind=bf16),
        ],
        scratch_shapes=[
            pltpu.VMEM((64, 2048), bf16),
            pltpu.VMEM((2048, 128), bf16),
            pltpu.VMEM((2048, 128), bf16),
            pltpu.VMEM((2048, 128), bf16),
            pltpu.VMEM((2048, 128), bf16),
            pltpu.VMEM((32, 128, 128), f32),
            dma((23,)),
        ],
        compiler_params=params(10),
        name="rows",
    )(
        normed,
        *[
            hbm(v)
            for v in (
                step_proj.T,
                inner_proj,
                gate_proj,
                inner_other,
                gate_other,
                out_proj,
                out_other,
                saved,
            )
        ],
    )
    partial = pl.pallas_call(
        main_kernel,
        in_specs=[whole()] * 10,
        out_specs=anywhere,
        out_shape=pltpu.HBM((128, 2176), bf16),
        scratch_shapes=[
            pltpu.VMEM((2, 128, 128), f32),
            pltpu.VMEM((1, 128, 128), f32),
            pltpu.VMEM((4, 128, 128), f32),
            pltpu.VMEM((128, 2176), bf16),
            dma((4,)),
        ],
        compiler_params=params(6),
        name="main",
    )(own_rows, near_rows, rows, mix, derived_twin, proj_v, low_v, held, low_twin, vec)
    arrived = lax.all_to_all(partial.reshape(16, 8, 2176), "kv", 0, 0, tiled=True)
    base = pl.pallas_call(
        state_kernel,
        in_specs=[anywhere] * 2 + [whole()] * 2,
        out_specs=anywhere,
        out_shape=shape(64, 128, 128),
        scratch_shapes=[
            pltpu.VMEM((64, 128, 128), f32),
            pltpu.VMEM((64, 128, 128), f32),
            dma((8,)),
            dma((8,)),
        ],
        compiler_params=params(12),
        name="state",
    )(hbm(saved), hbm(partial), held, mix)
    mixed = pl.pallas_call(
        sum_kernel,
        in_specs=[whole()],
        out_specs=whole(),
        out_shape=shape(8, 2048, kind=bf16),
        compiler_params=params(4),
        name="total",
    )(arrived)
    return mixed, base.reshape(64, 2, 64, 128)


def solution(mesh):
    both = ("kv", "tp")
    placed = (
        P(("dp", "kv", "tp"), None),
        P(),
        P(None, both),
        P(None, both),
        P(None, both),
        P(None, both),
        P(),
        P(),
        P(),
        P(),
        P(),
        P(),
        P(),
        P(),
        P(both, None),
        P("dp", both, None, None),
        P("dp", None, both),
        P("dp", None, both),
        P("dp", None, both),
        P("dp", None, both),
        P("dp"),
    )
    return jax.shard_map(
        body,
        mesh=mesh,
        in_specs=placed,
        out_specs=(P(("dp", "kv", "tp"), None), P("dp", both, None, None)),
        check_vma=False,
    )
```

```python
import jax
import jax.numpy as jnp
from jax import lax
from jax.experimental import pallas as pl
from jax.experimental.pallas import tpu as pltpu
from jax.sharding import PartitionSpec as P


EPSILON = 0.1
INNER = 4096
f32 = jnp.float32
bf16 = jnp.bfloat16
NT = (((1,), (1,)), ((), ()))
NN = (((1,), (0,)), ((), ()))


def dot(a, b, dims=NN):
    return lax.dot_general(a, b, dims, preferred_element_type=f32)


def silu(x):
    return x * (1.0 / (1.0 + jnp.exp(-x)))


def fetch(pairs, sems):
    copies = [pltpu.make_async_copy(src, dst, sems.at[k]) for k, (src, dst) in enumerate(pairs)]
    for copy in copies:
        copy.start()
    return copies


def device_rank():
    return lax.axis_index("kv") * 2 + lax.axis_index("tp")


def begin_kernel(
    tok_hbm, w_hbm, r_hbm, wh_hbm, rh_hbm, all_hbm, out_ref, hist_ref, tok_s, wh_s, rh_s, sems, sent
):
    copies = fetch(
        (
            (tok_hbm, tok_s),
            (wh_hbm, wh_s),
            (rh_hbm, rh_s),
            (w_hbm, out_ref.at[0:32]),
            (r_hbm, out_ref.at[32:64]),
        ),
        sems,
    )
    copies[0].wait()
    out = fetch([(tok_s, all_hbm.at[k]) for k in range(16)], sent)
    copies[1].wait()
    copies[2].wait()
    for t in range(7):
        both = jnp.concatenate([wh_s[t].astype(f32), rh_s[t].astype(f32)], axis=1).astype(bf16)
        out_ref[64:80, t * 128 : (t + 1) * 128] = both[0:16]
        out_ref[64:80, (7 + t) * 128 : (8 + t) * 128] = both[16:32]
    out_ref[64:80, 1792:2048] = jnp.zeros((16, 256), bf16)
    hist_ref[...] = out_ref[64:80, :]
    for copy in copies[3:] + out:
        copy.wait()


def windows(rows, acc):
    out = []
    for j in range(3):
        w = rows[j]
        for a in range(1, 5):
            w = jnp.where(acc == a, rows[a + j], w)
        out.append(w)
    return out


def old_parts(taps, w):
    return (
        taps[0] * w[0] + taps[1] * w[1] + taps[2] * w[2],
        taps[0] * w[1] + taps[1] * w[2],
        taps[0] * w[2],
    )


def prep_kernel(
    saved_hbm,
    ihist_hbm,
    tin_hbm,
    tw_hbm,
    tr_hbm,
    gain_hbm,
    ls_hbm,
    acc_hbm,
    decay_hbm,
    skip_hbm,
    bias_hbm,
    give_hbm,
    held_s,
    acc_ref,
    vec_ref,
    sent_ref,
    low_s,
    saved_s,
    ihist_s,
    tin_s,
    twin_s,
    tw_s,
    tr_s,
    gain_s,
    twin_gain_s,
    ls_s,
    acc_s,
    heads_s,
    sems,
    sent,
):
    rank = device_rank()
    core = rank & 1
    head = rank * 2
    col = pl.multiple_of(rank * 128, 128)
    twin_col = pl.multiple_of((rank ^ 1) * 128, 128)
    group = pl.multiple_of((rank >> 2) * 128, 128)
    small = (
        (acc_hbm, acc_s),
        (ls_hbm, ls_s),
        (decay_hbm, heads_s.at[0:1]),
        (skip_hbm, heads_s.at[1:2]),
        (bias_hbm, heads_s.at[2:3]),
        (tin_hbm.at[:, pl.ds(col, 128)], tin_s),
        (tin_hbm.at[:, pl.ds(twin_col, 128)], twin_s),
        (tw_hbm.at[:, pl.ds(group, 128)], tw_s),
        (tr_hbm.at[:, pl.ds(group, 128)], tr_s),
        (gain_hbm.at[:, pl.ds(col, 128)], gain_s),
        (gain_hbm.at[:, pl.ds(twin_col, 128)], twin_gain_s),
        (ihist_hbm, ihist_s),
    )
    big = tuple(
        (saved_hbm.at[pl.ds(kv * 4 + (1 - core) * 2, 2)], saved_s.at[kv * 2 : kv * 2 + 2])
        for kv in range(16)
    )
    copies = fetch(big + small, sems)
    out = []
    for k in range(4):
        block = slice(k * 8, (k + 1) * 8)
        for copy in copies[k * 4 : k * 4 + 4]:
            copy.wait()
        low_s[block] = saved_s[block].astype(bf16)
        out.append(pltpu.make_async_copy(low_s.at[block], give_hbm.at[block], sent.at[k]))
        out[-1].start()
    for copy in copies[len(big) :]:
        copy.wait()

    tin = tin_s[...].astype(f32)
    vec_ref[0:4, :] = tin
    vec_ref[4:8, :] = tw_s[...].astype(f32)
    vec_ref[8:12, :] = tr_s[...].astype(f32)
    place = lax.broadcasted_iota(jnp.int32, (1, 64), 1)
    first = lax.broadcasted_iota(jnp.int32, (1, 128), 1) < 64

    twin_head = (rank ^ 1) * 2

    def of_head(k, h):
        return jnp.sum(jnp.where(place == h, heads_s[k : k + 1], 0.0), axis=-1, keepdims=True)

    def spread(k, h):
        return jnp.where(first, of_head(k, h), of_head(k, h + 1))

    vec_ref[12:13, :] = -jnp.exp(spread(0, head))
    vec_ref[13:14, :] = spread(1, head)
    vec_ref[14:15, :] = spread(2, head)
    vec_ref[15:16, :] = gain_s[...]
    vec_ref[16:20, :] = twin_s[...].astype(f32)
    vec_ref[20:21, :] = -jnp.exp(spread(0, twin_head))
    vec_ref[21:22, :] = spread(1, twin_head)
    vec_ref[22:23, :] = spread(2, twin_head)
    vec_ref[23:24, :] = twin_gain_s[...]

    acc_row = acc_s[...]
    acc = jnp.broadcast_to(acc_row.astype(f32), (128, 64)).T
    acc_ref[...] = acc
    rows = [ihist_s[t].astype(f32) for t in range(7)]
    taps = [tin[k : k + 1] for k in range(4)]
    for i, part in enumerate(old_parts(taps, windows(rows, acc))):
        held_s[4 + i] = part

    def wide(pair):
        return jnp.concatenate([jnp.broadcast_to(v, (64, 64)) for v in pair], axis=0).T

    weights = [[], [], [], []]
    totals = []
    for h in range(2):
        rate = -jnp.exp(of_head(0, head + h))
        steps = [ls_s[t, h : h + 1, :] for t in range(4)]
        keep = [(acc_row > t).astype(f32) for t in range(4)]
        logs = [rate * steps[t] * keep[t] for t in range(4)]
        tail = jnp.zeros((1, 64), f32)
        for t in (3, 2, 1, 0):
            weights[t].append(keep[t] * jnp.exp(tail) * steps[t])
            tail = tail + logs[t]
        totals.append(jnp.exp(tail))
    held_s[7] = wide(totals)
    for t in range(4):
        held_s[t] = silu(sum(taps[k] * rows[t + k] for k in range(4))) * wide(weights[t])

    for q in range(2):
        start = (1 - core) * 2 + q
        block = slice(q * 16, (q + 1) * 16)
        for t in range(8):
            sent_ref[t, block] = held_s[t, pl.ds(start, 16, stride=4), :]
    for copy in out:
        copy.wait()


def group_kernel(own_ref, twin_ref, near_ref, far_ref, acc_ref, vec_ref, mix_s, hist_s):
    member = device_rank() & 3
    pieces = (own_ref.at[64:80], twin_ref.at[64:80], near_ref, far_ref)
    for x, p in enumerate(pieces):
        at = pl.multiple_of((member ^ x) * 32, 32)
        for t in range(7):
            hist_s[t, pl.ds(at, 16), :] = p[:, t * 128 : (t + 1) * 128].astype(f32)
            hist_s[t, pl.ds(at + 16, 16), :] = p[:, (7 + t) * 128 : (8 + t) * 128].astype(f32)
    both = [hist_s[t].T for t in range(7)]
    acc = acc_ref[...]
    acc2 = jnp.concatenate([acc, acc], axis=0)
    taps = [
        jnp.concatenate(
            [
                jnp.broadcast_to(vec_ref[4 + k : 5 + k, :], (64, 128)),
                jnp.broadcast_to(vec_ref[8 + k : 9 + k, :], (64, 128)),
            ],
            axis=0,
        )
        for k in range(4)
    ]
    for i, part in enumerate(old_parts(taps, windows(both, acc2))):
        mix_s[i] = part[0:64]
        mix_s[3 + i] = part[64:128]
    for t in range(4):
        w_old = silu(sum(vec_ref[4 + k : 5 + k, :] * both[t + k][0:64] for k in range(4)))
        mix_s[6 + t] = w_old.astype(bf16).astype(f32)


def state_kernel(
    saved_hbm, after_hbm, held_s, mix_s, base_hbm, saved_s, base_s, sems, sent
):
    blocks = [slice(k * 8, (k + 1) * 8) for k in range(8)]
    copies = fetch([(saved_hbm.at[k], saved_s.at[k]) for k in blocks], sems)
    tot = jnp.concatenate([held_s[7], held_s[7]], axis=0).T
    at = jnp.concatenate(
        [jnp.concatenate([held_s[2 * p], held_s[2 * p + 1]], axis=0).T for p in range(2)], axis=1
    ).astype(bf16)
    b = mix_s[6:10].reshape(256, 128).astype(bf16)
    lane = lax.broadcasted_iota(jnp.int32, (1, 256), 1) & 63
    out = []
    for k in range(8):
        copies[k].wait()
        for first in range(k * 8, (k + 1) * 8, 4):
            parts = [at * (lane == first + q).astype(f32).astype(bf16) for q in range(4)]
            new = dot(jnp.concatenate(parts, axis=0), b)
            for q in range(4):
                s = first + q
                base_s[s] = saved_s[s] * tot[:, s : s + 1] + new[q * 128 : (q + 1) * 128]
        copy = pltpu.make_async_copy(base_s.at[blocks[k]], base_hbm.at[blocks[k]], sent.at[k])
        copy.start()
        out.append(copy)
    for copy in out:
        copy.wait()


def rounded(v):
    return v.astype(bf16).astype(f32)


def norm_kernel(mine_ref, norm_ref, own_ref, twin_ref, nrm_ref, rows_ref, wall_s):
    core = lax.axis_index("tp")
    for c, p in ((core, own_ref), (1 - core, twin_ref)):
        at = pl.multiple_of(c * 32, 32)
        wall_s[pl.ds(at, 32), :] = p[0:32, :]
        wall_s[pl.ds(64 + at, 32), :] = p[32:64, :]
    gain = norm_ref[...]
    for k in range(8):
        x = mine_ref[2 * k : 2 * k + 2].astype(f32).reshape(16, 2048)
        scale = lax.rsqrt(jnp.mean(x * x, axis=-1, keepdims=True) + EPSILON)
        nrm_ref[k * 16 : (k + 1) * 16, :] = (x * scale * gain).astype(bf16)
    rows_ref[...] = dot(nrm_ref[...], wall_s[...], NT).astype(bf16)


def rows_kernel(
    nrm_ref,
    step_hbm,
    inner_hbm,
    gate_hbm,
    twin_inner_hbm,
    twin_gate_hbm,
    own_hbm,
    twin_own_hbm,
    saved_hbm,
    rows_ref,
    proj_ref,
    low_ref,
    step_s,
    inner_s,
    gate_s,
    twin_inner_s,
    twin_gate_s,
    low_s,
    sems,
):
    core = lax.axis_index("tp")
    copies = fetch(
        (
            (step_hbm, step_s),
            (inner_hbm, inner_s),
            (gate_hbm, gate_s),
            (twin_inner_hbm, twin_inner_s),
            (twin_gate_hbm, twin_gate_s),
        )
        + tuple(
            (saved_hbm.at[pl.ds(kv * 4 + core * 2, 2)], low_s.at[kv * 2 : kv * 2 + 2])
            for kv in range(16)
        )
        + ((own_hbm, proj_ref.at[0]), (twin_own_hbm, proj_ref.at[1])),
        sems,
    )
    normed = nrm_ref[...]
    for copy in copies[0:5]:
        copy.wait()
    weights = [inner_s[...], twin_inner_s[...], gate_s[...], twin_gate_s[...]]
    both = rounded(dot(normed, jnp.concatenate(weights, axis=1)))
    for k in range(4):
        rows_ref[2 + k] = both[:, k * 128 : (k + 1) * 128]
    both = dot(normed, step_s[...], NT)
    lane = lax.broadcasted_iota(jnp.int32, (64, 256), 1)
    head = (device_rank() ^ (lane >> 7)) * 2 + ((lane >> 6) & 1)
    pick = lax.broadcasted_iota(jnp.int32, (64, 256), 0) == head
    pick = pick.astype(f32).astype(bf16)
    high = both.astype(bf16)
    rest = both - high.astype(f32)
    mid = rest.astype(bf16)
    low = (rest - mid.astype(f32)).astype(bf16)
    both = dot(high, pick) + (dot(mid, pick) + dot(low, pick))
    rows_ref[0] = both[:, 0:128]
    rows_ref[1] = both[:, 128:256]
    for copy in copies[5:21]:
        copy.wait()
    low_ref[...] = low_s[...].astype(bf16)
    for copy in copies[21:]:
        copy.wait()


def main_kernel(
    own_rows_ref,
    near_rows_ref,
    rows_s,
    mix_s,
    got_ref,
    proj_s,
    low_s,
    held_s,
    twin_low_ref,
    vec_ref,
    out_hbm,
    pair_s,
    read_s,
    part_s,
    out_s,
    sent,
):
    core = lax.axis_index("tp")
    lower = (lax.axis_index("kv") & 1) == 0
    half = lax.broadcasted_iota(jnp.int32, (128, 128), 1) < 64
    own = own_rows_ref[...].astype(f32)
    near = near_rows_ref[...].astype(f32)
    left = jnp.where(lower, own, near)
    right = jnp.where(lower, near, own)
    pair_s[0] = jnp.where(half, left, pltpu.roll(right, 64, 1))
    pair_s[1] = jnp.where(half, pltpu.roll(left, 64, 1), right)

    def at_time(ref, t, k):
        return jnp.concatenate([ref[k, pl.ds(q * 4 + t, 16, stride=8), :] for q in range(2)], axis=0)

    def put(ref, t, k, value):
        for q in range(2):
            ref[k, pl.ds(q * 4 + t, 16, stride=8), :] = value[q * 16 : (q + 1) * 16]

    def chosen(ref, k):
        return jnp.concatenate(
            [ref[k, pl.ds(core * 2 + q, 16, stride=4), :] for q in range(2)], axis=0
        )

    def conv_new(new, parts, taps):
        out = []
        for i in range(4):
            v = taps[3] * new[i]
            for d in range(1, i + 1):
                v = v + taps[3 - d] * new[i - d]
            out.append(silu(v if i == 3 else v + parts[i]))
        return out

    def taps_of(first):
        return [vec_ref[first + k : first + k + 1, :] for k in range(4)]

    def mixing(k, base, taps):
        new = [at_time(pair_s, t, k) for t in range(4)]
        return [rounded(v) for v in conv_new(new, [chosen(mix_s, base + i) for i in range(3)], taps)]

    write = mixing(0, 0, taps_of(4))
    read = mixing(1, 3, taps_of(8))
    for t in range(4):
        put(read_s, t, 0, read[t])

    def score(x, y):
        return jnp.sum(x * y, axis=-1, keepdims=True)

    scores = [[score(read[i], write[j]) for j in range(i + 1)] for i in range(4)]
    past = [chosen(mix_s, 6 + t) for t in range(4)]
    olds = [[score(read[i], past[t]) for t in range(4)] for i in range(4)]
    for p in range(2):
        if p == 0:
            held = [chosen(held_s, t) for t in range(4)]
            parts = [chosen(held_s, 4 + t) for t in range(3)]
            tot = chosen(held_s, 7)
        else:
            held = [got_ref[t] for t in range(4)]
            parts = [got_ref[4 + t] for t in range(3)]
            tot = got_ref[7]
        inner = conv_new(
            [at_time(rows_s, t, 2 + p) for t in range(4)], parts, taps_of(16 if p else 0)
        )
        first = 20 if p else 12
        rate, skip, bias = (vec_ref[first + k : first + k + 1, :] for k in range(3))
        steps = []
        for t in range(4):
            z = at_time(rows_s, t, p) + bias
            steps.append(jnp.maximum(z, 0.0) + jnp.log1p(jnp.exp(-jnp.abs(z))))
        sums = [rate * steps[0]]
        for t in range(1, 4):
            sums.append(sums[-1] + rate * steps[t])
        moved = [steps[t] * inner[t] for t in range(4)]
        for i in range(4):
            decay = jnp.exp(sums[i])
            state = held[0] * olds[i][0]
            for t in range(1, 4):
                state = state + held[t] * olds[i][t]
            y = decay * state + skip * inner[i] + scores[i][i] * moved[i]
            for j in range(i):
                y = y + scores[i][j] * jnp.exp(sums[i] - sums[j]) * moved[j]
            gate = silu(at_time(rows_s, i, 4 + p))
            put(part_s, i, p, y * gate)
            put(part_s, i, 2 + p, decay * tot * gate)

    quarter = lax.broadcasted_iota(jnp.int32, (16, 128), 0) >> 2
    for g in range(8):
        rows = slice(g * 16, (g + 1) * 16)
        r = read_s[0, rows, :].astype(bf16)
        for p, low in enumerate((low_s, twin_low_ref)):
            full = dot(r, low[g * 4 : (g + 1) * 4].reshape(512, 128), NT)
            v = full[:, 0:128]
            for q in range(1, 4):
                v = jnp.where(quarter == q, full[:, q * 128 : (q + 1) * 128], v)
            part_s[p, rows, :] = part_s[p, rows, :] + part_s[2 + p, rows, :] * v

    lane = lax.broadcasted_iota(jnp.int32, (128, 128), 1)
    gated = [part_s[p] for p in range(2)]
    sq = jnp.sum(gated[0] * gated[0] + gated[1] * gated[1], axis=-1, keepdims=True)
    hi = rounded(sq)
    out_s[:, 2048:2176] = jnp.where(lane == 0, hi, jnp.where(lane == 1, sq - hi, 0.0)).astype(bf16)
    unscaled = [
        (gated[p] * vec_ref[15 + 8 * p : 16 + 8 * p, :]).astype(bf16) for p in range(2)
    ]
    out = []
    for k in range(4):
        cols = slice(k * 512, (k + 1) * 512)
        value = dot(unscaled[0], proj_s[0, :, cols]) + dot(unscaled[1], proj_s[1, :, cols])
        out_s[:, cols] = value.astype(bf16)
        cols = slice(k * 512, 2176 if k == 3 else (k + 1) * 512)
        out.append(pltpu.make_async_copy(out_s.at[:, cols], out_hbm.at[:, cols], sent.at[k]))
        out[-1].start()
    for copy in out:
        copy.wait()


def sum_kernel(in_ref, out_ref):
    total = in_ref[0].astype(f32)
    for k in range(1, 16):
        total = total + in_ref[k].astype(f32)
    squares = jnp.sum(total[:, 2048:2176], axis=-1, keepdims=True)
    out_ref[...] = (total[:, 0:2048] * lax.rsqrt(squares / INNER + EPSILON)).astype(bf16)


def whole(memory_space=pltpu.VMEM):
    return pl.BlockSpec(memory_space=memory_space)


def swapped(value, axis):
    return lax.ppermute(value, axis, [(k, k ^ 1) for k in range(lax.axis_size(axis))])


def params(mib, **kw):
    return pltpu.CompilerParams(vmem_limit_bytes=mib << 20, **kw)


def body(
    tokens,
    norm_gain,
    gate_proj,
    inner_proj,
    write_proj,
    read_proj,
    step_proj,
    step_bias,
    decay_log,
    skip_gain,
    conv_inner,
    conv_write,
    conv_read,
    out_gain,
    out_proj,
    saved_state,
    inner_history,
    write_history,
    read_history,
    last_steps,
    accepted,
):
    def hbm(value):
        return pltpu.with_memory_space_constraint(value, pltpu.HBM)

    anywhere = whole(pl.ANY)
    dma = pltpu.SemaphoreType.DMA

    def shape(*dims, kind=f32):
        return jax.ShapeDtypeStruct(dims, kind)

    saved = saved_state.reshape(64, 128, 128)
    sent, pack, hist = pl.pallas_call(
        begin_kernel,
        out_shape=[
            pltpu.HBM((16, 8, 2048), bf16),
            shape(80, 2048, kind=bf16),
            shape(16, 2048, kind=bf16),
        ],
        in_specs=[anywhere] * 5,
        out_specs=[anywhere, whole(), whole()],
        scratch_shapes=[
            pltpu.VMEM((8, 2048), bf16),
            pltpu.VMEM((7, 32, 64), bf16),
            pltpu.VMEM((7, 32, 64), bf16),
            dma((5,)),
            dma((16,)),
        ],
        compiler_params=params(4),
        name="begin",
    )(
        hbm(tokens),
        hbm(write_proj.T),
        hbm(read_proj.T),
        hbm(write_history.transpose(1, 2, 0)),
        hbm(read_history.transpose(1, 2, 0)),
    )
    mine = lax.all_to_all(sent, "kv", 0, 0, tiled=True)
    hist_kv = swapped(hist, "kv")
    pack_tp = swapped(pack, "tp")
    hist_both = swapped(hist_kv, "tp")
    gate_other = swapped(gate_proj, "tp")
    inner_other = swapped(inner_proj, "tp")
    out_other = swapped(out_proj, "tp")

    give, held, acc, vec, derived = pl.pallas_call(
        prep_kernel,
        in_specs=[anywhere] * 11,
        out_specs=[anywhere] + [whole()] * 4,
        out_shape=[
            pltpu.HBM((32, 128, 128), bf16),
            shape(8, 64, 128),
            shape(64, 128),
            shape(24, 128),
            shape(8, 32, 128),
        ],
        scratch_shapes=[
            pltpu.VMEM((32, 128, 128), bf16),
            pltpu.VMEM((32, 128, 128), f32),
            pltpu.VMEM((7, 64, 128), bf16),
            pltpu.VMEM((4, 128), bf16),
            pltpu.VMEM((4, 128), bf16),
            pltpu.VMEM((4, 128), bf16),
            pltpu.VMEM((4, 128), bf16),
            pltpu.VMEM((1, 128), f32),
            pltpu.VMEM((1, 128), f32),
            pltpu.VMEM((4, 2, 64), f32),
            pltpu.VMEM((1, 64), jnp.int32),
            pltpu.VMEM((3, 64), f32),
            dma((28,)),
            dma((4,)),
        ],
        compiler_params=params(12),
        name="prep",
    )(
        *[
            hbm(v)
            for v in (
                saved,
                inner_history.transpose(1, 0, 2),
                conv_inner,
                conv_write,
                conv_read,
                out_gain[None, :],
                last_steps.transpose(1, 2, 0),
                accepted[None, :],
                decay_log[None, :],
                skip_gain[None, :],
                step_bias[None, :],
            )
        ]
    )
    mix = pl.pallas_call(
        group_kernel,
        in_specs=[whole()] * 6,
        out_specs=whole(),
        out_shape=shape(10, 64, 128),
        scratch_shapes=[pltpu.VMEM((7, 128, 128), f32)],
        compiler_params=params(6),
        name="group",
    )(pack, pack_tp, hist_kv, hist_both, acc, vec)

    derived_twin = swapped(derived, "tp")
    low_twin = swapped(give, "tp")
    normed, own_rows = pl.pallas_call(
        norm_kernel,
        in_specs=[whole()] * 4,
        out_specs=[whole()] * 2,
        out_shape=[shape(128, 2048, kind=bf16), shape(128, 128, kind=bf16)],
        scratch_shapes=[pltpu.VMEM((128, 2048), bf16)],
        compiler_params=params(6),
        name="norm",
    )(mine, norm_gain[None, :], pack, pack_tp)
    near_rows = swapped(own_rows, "kv")
    rows, proj_v, low_v = pl.pallas_call(
        rows_kernel,
        in_specs=[whole()] + [anywhere] * 8,
        out_specs=[whole()] * 3,
        out_shape=[
            shape(6, 128, 128),
            shape(2, 128, 2048, kind=bf16),
            shape(32, 128, 128, kind=bf16),
        ],
        scratch_shapes=[
            pltpu.VMEM((64, 2048), bf16),
            pltpu.VMEM((2048, 128), bf16),
            pltpu.VMEM((2048, 128), bf16),
            pltpu.VMEM((2048, 128), bf16),
            pltpu.VMEM((2048, 128), bf16),
            pltpu.VMEM((32, 128, 128), f32),
            dma((23,)),
        ],
        compiler_params=params(10),
        name="rows",
    )(
        normed,
        *[
            hbm(v)
            for v in (
                step_proj.T,
                inner_proj,
                gate_proj,
                inner_other,
                gate_other,
                out_proj,
                out_other,
                saved,
            )
        ],
    )
    partial = pl.pallas_call(
        main_kernel,
        in_specs=[whole()] * 10,
        out_specs=anywhere,
        out_shape=pltpu.HBM((128, 2176), bf16),
        scratch_shapes=[
            pltpu.VMEM((2, 128, 128), f32),
            pltpu.VMEM((1, 128, 128), f32),
            pltpu.VMEM((4, 128, 128), f32),
            pltpu.VMEM((128, 2176), bf16),
            dma((4,)),
        ],
        compiler_params=params(6),
        name="main",
    )(own_rows, near_rows, rows, mix, derived_twin, proj_v, low_v, held, low_twin, vec)
    arrived = lax.all_to_all(partial.reshape(16, 8, 2176), "kv", 0, 0, tiled=True)
    base = pl.pallas_call(
        state_kernel,
        in_specs=[anywhere] * 2 + [whole()] * 2,
        out_specs=anywhere,
        out_shape=shape(64, 128, 128),
        scratch_shapes=[
            pltpu.VMEM((64, 128, 128), f32),
            pltpu.VMEM((64, 128, 128), f32),
            dma((8,)),
            dma((8,)),
        ],
        compiler_params=params(12),
        name="state",
    )(hbm(saved), hbm(partial), held, mix)
    mixed = pl.pallas_call(
        sum_kernel,
        in_specs=[whole()],
        out_specs=whole(),
        out_shape=shape(8, 2048, kind=bf16),
        compiler_params=params(4),
        name="total",
    )(arrived)
    return mixed, base.reshape(64, 2, 64, 128)


def solution(mesh):
    both = ("kv", "tp")
    placed = (
        P(("dp", "kv", "tp"), None),
        P(),
        P(None, both),
        P(None, both),
        P(None, both),
        P(None, both),
        P(),
        P(),
        P(),
        P(),
        P(),
        P(),
        P(),
        P(),
        P(both, None),
        P("dp", both, None, None),
        P("dp", None, both),
        P("dp", None, both),
        P("dp", None, both),
        P("dp", None, both),
        P("dp"),
    )
    return jax.shard_map(
        body,
        mesh=mesh,
        in_specs=placed,
        out_specs=(P(("dp", "kv", "tp"), None), P("dp", both, None, None)),
        check_vma=False,
    )
```
